512 devices in a mesh: sp: 64 (over z, y), tp: 8 (over x, core).
Axes of the slice: x: 4, y: 8, z: 8, core: 2. Of those that a mesh axis runs over, the one named last changes fastest.
Arguments:
- inputs: bfloat16 [16384, 2048], P('sp', 'tp'), may hold values from -200 to 200
- input_gain: bfloat16 [2048], P('tp'), may hold values from 0.099609375 to 1.8984375
- stick_query_w: bfloat16 [2048, 1024], P(None, 'tp'), may hold values from -0.3125 to 0.3125
- stick_key_w: bfloat16 [2048, 1024], P(None, 'tp'), may hold values from -0.125 to 0.125
- stick_value_w: bfloat16 [2048, 1024], P(None, 'tp'), may hold values from -0.125 to 0.125
- ret_query_w: bfloat16 [2048, 2048], P(None, 'tp'), may hold values from -0.125 to 0.125
- ret_key_w: bfloat16 [2048, 2048], P(None, 'tp'), may hold values from -0.125 to 0.125
- ret_value_w: bfloat16 [2048, 2048], P(None, 'tp'), may hold values from -0.125 to 0.125
- stick_offset: float32 [8], P('tp'), may hold values from -17 to -2
- ret_log_decay: float32 [8], P('tp'), may hold values from -0.04 to 0, as said below
- initial_state: float32 [8, 256, 256], P('tp', 'sp'), may hold values from -76.8 to 76.8
- stick_gain: float32 [1024], P('tp'), may hold values from 0.1 to 1.9
- ret_gain: float32 [2048], P('tp'), may hold values from 0.1 to 1.9
- stick_out_w: bfloat16 [1024, 2048], P('tp', 'sp'), may hold values from -0.125 to 0.125
- ret_out_w: bfloat16 [2048, 2048], P('tp', 'sp'), may hold values from -0.09375 to 0.09375
Outputs:
- layer_out: bfloat16 [16384, 2048], P(('sp', 'tp'))
The draws below stay inside these ranges and needn't reach their ends.
Inputs may be any that keep to these rules, and one draw needn't show every extreme that they name: `ret_log_decay`: every entry is negative.
All inputs are finite; a program needn't handle non-finite values.
Results may differ from the reference program's by a relative error of at most 0.017.
Values may be sent and summed in bfloat16 or wider, within the bound.
No kernel may reach another device: no remote copies, remote signals or barrier semaphores. Data moves between devices by JAX's collectives and lax.ppermute only.
A program may use at most 64 MiB of HBM per device.

```python
import math
import jax
import jax.numpy as jnp
from jax import lax

D = 2048
STICK_HEADS = 8
STICK_DIM = 128
RET_HEADS = 8
RET_DIM = 256
TOKENS = 16384
N_TP = 8


def draw_inputs(key, part):
    base_key, row_key, col_key = jax.random.split(jax.random.fold_in(key, 11), 3)
    base = jax.random.normal(base_key, (TOKENS, D), jnp.float32)
    position_ramp = jnp.arange(D, dtype=jnp.float32) / D
    roughness = jax.random.uniform(col_key, (D,), jnp.float32, 0.5, 1.5)
    row_scale = jnp.exp(jax.random.uniform(row_key, (TOKENS, 1), jnp.float32, 0.0, 2.3))
    col_scale = 3.0 ** position_ramp * roughness
    values = row_scale * base * col_scale[None, :]
    return jnp.clip(values, -200.0, 200.0).astype(jnp.bfloat16)


def draw_stick_offset(key, part):
    order_key, near_key, far_key = jax.random.split(jax.random.fold_in(key, 23), 3)
    ranking = jax.random.permutation(order_key, STICK_HEADS)
    fast_heads = ranking < STICK_HEADS // 2
    near_offset = -jnp.log(40.0) - 3.1 + jax.random.uniform(near_key, (STICK_HEADS,), jnp.float32, -0.5, 0.5)
    far_offset = -jnp.log(TOKENS * 1.0) - 3.1 - jax.random.uniform(far_key, (STICK_HEADS,), jnp.float32, 0.0, 1.5)
    return jnp.where(fast_heads, near_offset, far_offset).astype(jnp.float32)


def draw_ret_log_decay(key, part):
    order_key, quick_key, slow_key = jax.random.split(jax.random.fold_in(key, 37), 3)
    ranking = jax.random.permutation(order_key, RET_HEADS)
    fast_heads = ranking < RET_HEADS // 2
    quick_decay = -jax.random.uniform(quick_key, (RET_HEADS,), jnp.float32, 0.01, 0.034)
    slow_decay = -jax.random.uniform(slow_key, (RET_HEADS,), jnp.float32, 0.2, 1.5) / TOKENS
    return jnp.where(fast_heads, quick_decay, slow_decay).astype(jnp.float32)


def level_of(rng, extent, pieces, low, largest):
    def one(axis_at, blocks):
        steps = jax.random.uniform(jax.random.fold_in(jax.random.fold_in(rng, 6), axis_at), (blocks,), jnp.float32, low / len(pieces), largest / len(pieces))
        return jnp.repeat(jnp.exp(steps), extent[axis_at] // blocks).reshape((-1,) + (1,) * (len(extent) - axis_at - 1))

    gain = one(*pieces[0])
    for cut in pieces[1:]:
        gain = gain * one(*cut)
    return gain


def bell_draw(key, shape, scale, limit, shards=(), kind=jnp.bfloat16):
    gain = level_of(key, shape, shards, -0.22, 0.18) if shards else 1.0
    values = jax.random.normal(key, shape, jnp.float32) * scale * gain
    return jnp.minimum(jnp.maximum(values, -limit), limit).astype(kind)


def setup_inputs(seed: int = 0) -> dict:
    streams_of = jax.random.split(jax.random.key(seed), 16)
    return {
        "inputs": draw_inputs(jax.random.fold_in(streams_of[15], 71), 0),
        "input_gain": jnp.clip(1.0 + 0.18 * jax.random.normal(streams_of[1], (D,), jnp.float32), 0.099609375, 1.8984375).astype(jnp.bfloat16),
        "stick_query_w": bell_draw(streams_of[2], (D, STICK_HEADS * STICK_DIM), (D // 6) ** -0.5, 0.3125, ((1, 8),)),
        "stick_key_w": bell_draw(streams_of[3], (D, STICK_HEADS * STICK_DIM), D ** -0.5, 0.125, ((1, 8),)),
        "stick_value_w": bell_draw(streams_of[4], (D, STICK_HEADS * STICK_DIM), D ** -0.5, 0.125, ((1, 8),)),
        "ret_query_w": bell_draw(streams_of[5], (D, RET_HEADS * RET_DIM), D ** -0.5, 0.125, ((1, 8),)),
        "ret_key_w": bell_draw(streams_of[6], (D, RET_HEADS * RET_DIM), D ** -0.5, 0.125, ((1, 8),)),
        "ret_value_w": bell_draw(streams_of[7], (D, RET_HEADS * RET_DIM), D ** -0.5, 0.125, ((1, 8),)),
        "stick_offset": draw_stick_offset(jax.random.fold_in(streams_of[15], 71), 0),
        "ret_log_decay": draw_ret_log_decay(jax.random.fold_in(streams_of[15], 71), 0),
        "initial_state": bell_draw(streams_of[10], (RET_HEADS, RET_DIM, RET_DIM), (0.1 * TOKENS ** 0.5), 76.8, ((0, 8), (1, 64)), jnp.float32),
        "stick_gain": jnp.clip(1.0 + 0.18 * jax.random.normal(streams_of[11], (STICK_HEADS * STICK_DIM,), jnp.float32), 0.1, 1.9),
        "ret_gain": jnp.clip(1.0 + 0.18 * jax.random.normal(streams_of[12], (RET_HEADS * RET_DIM,), jnp.float32), 0.1, 1.9),
        "stick_out_w": bell_draw(streams_of[13], (STICK_HEADS * STICK_DIM, D), (2 * STICK_HEADS * STICK_DIM) ** -0.5, 0.125, ((0, 8), (1, 64))),
        "ret_out_w": bell_draw(streams_of[14], (RET_HEADS * RET_DIM, D), (2 * RET_HEADS * RET_DIM) ** -0.5, 0.09375, ((0, 8), (1, 64))),
    }


epsilon = 1e-06
rope_base = 10000.0

def rotate(values, positions):
    half_width = values.shape[-1] // 2
    inverse = rope_base ** (-jnp.arange(half_width, dtype=jnp.float32) / half_width)
    angles = positions.astype(jnp.float32)[:, None] * inverse[None, :]
    cosine = jnp.cos(angles)[:, None, :]
    sine_table = jnp.sin(angles)[:, None, :]
    first_half = values[..., :half_width]
    second_half = values[..., half_width:]
    return jnp.concatenate([first_half * cosine - second_half * sine_table, second_half * cosine + first_half * sine_table], axis=-1)

def stick_head(packed):
    queries, key_table, value_table, offset = packed
    length = queries.shape[0]
    block_len = math.gcd(length, 1024)
    score_scale = queries.shape[1] ** (-0.5)

    def one_block(block_index):
        query_start = block_index * block_len
        query_rows = lax.dynamic_slice_in_dim(queries, query_start, block_len, 0)
        query_pos = query_start + jnp.arange(block_len, dtype=jnp.int32)

        def advance(turn_index, start_carry):
            running, before = start_carry
            key_start = (block_index - turn_index) * block_len
            key_rows = lax.dynamic_slice_in_dim(key_table, key_start, block_len, 0)
            value_rows = lax.dynamic_slice_in_dim(value_table, key_start, block_len, 0)
            key_pos = key_start + jnp.arange(block_len, dtype=jnp.int32)
            scores = jnp.dot(query_rows, key_rows.T, preferred_element_type=jnp.float32) * score_scale + offset
            allowed = key_pos[None, :] < query_pos[:, None]
            remain = jnp.where(allowed, jax.nn.log_sigmoid(-scores), 0.0)
            suffix = lax.cumsum(remain, axis=1, reverse=True) - remain + before[:, None]
            weights = jnp.where(allowed, jnp.exp(jax.nn.log_sigmoid(scores) + suffix), 0.0).astype(jnp.bfloat16)
            running = running + jnp.dot(weights, value_rows, preferred_element_type=jnp.float32)
            return (running, before + lax.optimization_barrier(jnp.sum(remain, axis=1)))
        start_carry = (jnp.zeros((block_len, value_table.shape[1]), jnp.float32), jnp.zeros((block_len,), jnp.float32))
        running, _ = lax.fori_loop(0, block_index + 1, advance, start_carry)
        return running
    return lax.map(one_block, jnp.arange(length // block_len, dtype=jnp.int32))

def retention(queries, key_table, value_table, log_decay, initial_state):
    length, head_count, ret_width = queries.shape
    block_len = math.gcd(length, 256)
    count_blocks = length // block_len
    local_pos = jnp.arange(block_len, dtype=jnp.float32)
    distance = local_pos[:, None] - local_pos[None, :]
    decay_mask = jnp.where(distance[None] >= 0.0, jnp.exp(log_decay[:, None, None] * jnp.maximum(distance, 0.0)[None]), 0.0)
    query_decay = jnp.exp(log_decay[None, :] * (local_pos[:, None] + 1.0))
    key_decay = jnp.exp(log_decay[None, :] * (block_len - 1.0 - local_pos[:, None]))
    block_decay = jnp.exp(log_decay * block_len)
    highest = lax.Precision.HIGHEST

    def advance(carried_state, blocks):
        query_block, key_block, value_block = blocks
        scores = jnp.einsum('thd,shd->hts', query_block, key_block, precision=highest) * decay_mask
        inner_part = jnp.einsum('hts,she->the', scores, value_block, precision=highest)
        cross_part = jnp.einsum('thd,hde->the', query_block, carried_state, precision=highest) * query_decay[:, :, None]
        carried_state = carried_state * block_decay[:, None, None] + jnp.einsum('shd,she->hde', key_block * key_decay[:, :, None], value_block, precision=highest)
        return (carried_state, inner_part + cross_part)
    blocks = tuple((array.reshape(count_blocks, block_len, head_count, ret_width) for array in (queries, key_table, value_table)))
    _, outputs = lax.scan(advance, initial_state, blocks)
    return outputs.reshape(length, head_count, ret_width)

def head_major(array, head_count):
    return jnp.transpose(array.reshape(array.shape[0], head_count, -1), (1, 0, 2))

def reference(inputs, input_gain, stick_query_w, stick_key_w, stick_value_w, ret_query_w, ret_key_w, ret_value_w, stick_offset, ret_log_decay, initial_state, stick_gain, ret_gain, stick_out_w, ret_out_w):
    length = inputs.shape[0]
    widened = inputs.astype(jnp.float32)
    row_scale = lax.rsqrt(lax.optimization_barrier(jnp.mean(widened * widened, axis=1)) + epsilon)
    scaled = (widened * input_gain.astype(jnp.float32)).astype(jnp.bfloat16)

    def project(weight):
        return (jnp.dot(scaled, weight, preferred_element_type=jnp.float32) * row_scale[:, None]).astype(jnp.bfloat16)
    stick_query = project(stick_query_w)
    stick_key = project(stick_key_w)
    stick_value = project(stick_value_w)
    ret_query = project(ret_query_w)
    ret_key = project(ret_key_w)
    ret_value = project(ret_value_w)
    stick_blocks = lax.map(stick_head, (head_major(stick_query, STICK_HEADS), head_major(stick_key, STICK_HEADS), head_major(stick_value, STICK_HEADS), stick_offset))
    stick_total = jnp.transpose(stick_blocks.reshape(STICK_HEADS, length, STICK_DIM), (1, 0, 2)).reshape(length, STICK_HEADS * STICK_DIM)
    stick_scale = lax.rsqrt(lax.optimization_barrier(jnp.mean(stick_total * stick_total, axis=1)) + epsilon)
    stick_normed = (stick_total * stick_scale[:, None] * stick_gain).astype(jnp.bfloat16)
    positions = jnp.arange(length, dtype=jnp.int32)
    turned_query = rotate(ret_query.reshape(length, RET_HEADS, RET_DIM).astype(jnp.float32), positions)
    turned_key = rotate(ret_key.reshape(length, RET_HEADS, RET_DIM).astype(jnp.float32), positions) * RET_DIM ** (-0.5)
    ret_values = ret_value.reshape(length, RET_HEADS, RET_DIM).astype(jnp.float32)
    ret_total = retention(turned_query, turned_key, ret_values, ret_log_decay, initial_state)
    centered = ret_total - lax.optimization_barrier(jnp.mean(ret_total, axis=2, keepdims=True))
    normed = centered * lax.rsqrt(lax.optimization_barrier(jnp.mean(centered * centered, axis=2, keepdims=True)) + epsilon)
    ret_normed = (normed.reshape(length, RET_HEADS * RET_DIM) * ret_gain).astype(jnp.bfloat16)
    stick_share = STICK_HEADS // N_TP * STICK_DIM
    ret_share = RET_HEADS // N_TP * RET_DIM
    layer_sum = jnp.zeros((length, D), jnp.float32)
    for run_index in range(N_TP):
        stick_cols = slice(run_index * stick_share, (run_index + 1) * stick_share)
        ret_cols = slice(run_index * ret_share, (run_index + 1) * ret_share)
        partial_value = jnp.dot(stick_normed[:, stick_cols], stick_out_w[stick_cols], preferred_element_type=jnp.float32)
        partial_value = partial_value + jnp.dot(ret_normed[:, ret_cols], ret_out_w[ret_cols], preferred_element_type=jnp.float32)
        rounded = lax.optimization_barrier(partial_value.astype(jnp.bfloat16))
        layer_sum = layer_sum + rounded.astype(jnp.float32)
    return layer_sum.astype(jnp.bfloat16)
```

```python
import functools

import jax
import jax.numpy as jnp
from jax import lax
from jax.experimental import pallas as pl
from jax.experimental.pallas import tpu as pltpu
from jax.sharding import Mesh
from jax.sharding import PartitionSpec as P

D = 2048
STICK_WIDTH = 1024
ROWS = 256
SD = 128
RD = 256
NZ = 8
NY = 8
SLICE = RD // NY
LOG2E = 1.4426950408889634

SP = ("z", "y")
TP = ("x", "c")
ALL = ("z", "y", "x", "c")

epsilon = 1e-06
rope_base = 10000.0
bf16 = jnp.bfloat16
f32 = jnp.float32

VMEM = pl.BlockSpec(memory_space=pltpu.VMEM)
SMEM = pl.BlockSpec(memory_space=pltpu.SMEM)


def mm(a, b, dims=((1,), (0,))):
    return lax.dot_general(a, b, (dims, ((), ())), preferred_element_type=f32)


def iota(shape, dim):
    return lax.broadcasted_iota(jnp.int32, shape, dim)


def slice_order():
    r = iota((RD, RD), 0)
    c = iota((RD, RD), 1)
    j, z, k = r // SLICE, (r % SLICE) // 4, r % 4
    return (c == SLICE * z + 4 * j + k).astype(f32).astype(bf16)


def call(kernel, out, in_specs, flops, scratch=()):
    return pl.pallas_call(
        kernel,
        out_shape=out,
        in_specs=in_specs,
        out_specs=jax.tree.map(lambda _: VMEM, out),
        scratch_shapes=list(scratch),
        compiler_params=pltpu.CompilerParams(vmem_limit_bytes=48 * 1024 * 1024),
        cost_estimate=pl.CostEstimate(flops=flops, bytes_accessed=1 << 20, transcendentals=0),
    )


def project_kernel(
    pos, lam, own, other, cos, sin, wsq, wsk, wsv, wrq, wrk, wrv, kvs, sq, tq, tk, rv
):
    core = pos[2]
    widths = (SD, SD, SD, RD, RD, RD)
    sums = [jnp.zeros((ROWS, w), f32) for w in widths]
    squares = jnp.zeros((ROWS, RD), f32)
    for part, ref in ((core, own), (1 - core, other)):
        for x in range(4):
            raw = ref[x, :ROWS, :].astype(f32)
            gain = ref[x, ROWS : ROWS + 1, :].astype(f32)
            squares = squares + raw * raw
            scaled = (raw * gain).astype(bf16)
            row = pl.multiple_of((2 * x + part) * RD, RD)
            for k, w in enumerate((wsq, wsk, wsv, wrq, wrk, wrv)):
                sums[k] = sums[k] + mm(scaled, w[pl.ds(row, RD), :])
    scale = lax.rsqrt(jnp.sum(squares, axis=1, keepdims=True) / D + epsilon)
    sq_v, sk_v, sv_v, rq_v, rk_v, rv_v = [(s * scale).astype(bf16) for s in sums]
    sq[...] = sq_v
    rv[...] = rv_v
    cosine, sine = cos[...], sin[...]
    half = RD // 2

    def turn(v):
        a, b = v[:, :half].astype(f32), v[:, half:].astype(f32)
        return jnp.concatenate([a * cosine - b * sine, b * cosine + a * sine], axis=1)

    tq[...] = turn(rq_v).astype(bf16)
    key = turn(rk_v) * (RD**-0.5)
    tk[...] = key.astype(bf16)
    left = (ROWS - 1 - iota((ROWS, RD), 0)).astype(f32)
    decayed = (key * jnp.exp(lam[0] * left)).astype(bf16)
    state = mm(decayed, rv_v, ((0,), (0,))).astype(bf16)
    ordered = mm(slice_order(), state).astype(bf16)
    for y in range(NY):
        kvs[y, :ROWS, :SD] = sk_v
        kvs[y, :ROWS, SD:] = sv_v
        kvs[y, ROWS:, :] = ordered[SLICE * y : SLICE * (y + 1), :]


def inner_kernel(lam, tq, tk, rv, inner):
    gap = (iota((ROWS, ROWS), 0) - iota((ROWS, ROWS), 1)).astype(f32)
    decay = jnp.where(gap >= 0.0, jnp.exp(lam[0] * jnp.maximum(gap, 0.0)), 0.0)
    scores = mm(tq[...], tk[...], ((1,), (1,))) * decay
    inner[...] = mm(scores.astype(bf16), rv[...])


def totals_kernel(lam, kvs, sq, init, out):
    step = jnp.exp(jnp.full((1, RD), lam[0] * ROWS, f32))
    run = jnp.zeros((SLICE, RD), f32)
    for y in range(NY):
        run = run * step + kvs[y, ROWS:, :].astype(f32)
    total = run.astype(bf16)
    first = init[...].astype(bf16)
    for z in range(NZ):
        out[z, :ROWS, :] = sq[...]
        out[z, ROWS : ROWS + SLICE, :] = total[:, :SD]
        out[z, ROWS + SLICE : ROWS + 2 * SLICE, :] = total[:, SD:]
        out[z, ROWS + 2 * SLICE :, :] = first


def entering_kernel(pos, lam, kvs, zq, out, start):
    mine = pos[0]
    step = jnp.exp(jnp.full((1, RD), lam[0] * ROWS, f32))
    row_step = jnp.exp(jnp.full((1, RD), lam[0] * (ROWS * NY), f32))
    top = ROWS + 2 * SLICE
    for z in range(NZ):
        both = zq[z, top : top + 8, :].astype(f32)
        start[4 * z : 4 * z + 4, :SD] = both[:4]
        start[4 * z : 4 * z + 4, SD:] = both[4:]
    before = start[...]
    for z in range(NZ):
        total = jnp.concatenate(
            [zq[z, ROWS : ROWS + SLICE, :], zq[z, ROWS + SLICE : ROWS + 2 * SLICE, :]], axis=1
        ).astype(f32)
        before = jnp.where(z < mine, before * row_step + total, before)
    run = before
    for y in range(NY):
        out[y, :, :] = run.astype(bf16)
        run = run * step + kvs[y, ROWS:, :].astype(f32)


def stick_kernel(pos, off, kvs, zq, out, acc, car, upper):
    mine, col = pos[0], pos[1]
    c1 = (SD**-0.5) * LOG2E
    c2 = off[0] * LOG2E
    upper[...] = (iota((ROWS, ROWS), 0) > iota((ROWS, ROWS), 1)).astype(f32).astype(bf16)

    def block(q, y, carry, total, masked):
        keys = kvs[y, :ROWS, :SD]
        values = kvs[y, :ROWS, SD:]
        s = mm(q, keys, ((1,), (1,))) * c1 + c2
        soft = jnp.maximum(s, 0.0) + jnp.log2(1.0 + jnp.exp2(-jnp.abs(s)))
        power = s - soft
        if masked:
            allowed = iota((ROWS, ROWS), 1) < iota((ROWS, ROWS), 0)
            soft = jnp.where(allowed, soft, 0.0)
        rounded = soft.astype(bf16)
        later = mm(rounded, upper[...])
        weight = jnp.exp2(power - later - carry)
        if masked:
            weight = jnp.where(allowed, weight, 0.0)
        total = total + mm(weight.astype(bf16), values)
        carry = carry + later[:, :1] + rounded[:, :1].astype(f32)
        return carry, total

    def finish(z, carry, total):
        out[z, :ROWS, :] = total.astype(bf16)
        wide = jnp.transpose(jnp.broadcast_to(carry, (ROWS, SD)))[:8, :]
        a, b = wide[:, :SD], wide[:, SD:]
        ha, hb = a.astype(bf16).astype(f32), b.astype(bf16).astype(f32)
        row = iota((8, SD), 0)
        packed = jnp.where(
            row == 0,
            ha,
            jnp.where(row == 1, hb, jnp.where(row == 2, a - ha, jnp.where(row == 3, b - hb, 0.0))),
        )
        out[z, ROWS:, :] = packed.astype(bf16)

    def nothing(z, _):
        out[z, :, :] = jnp.zeros((ROWS + 8, SD), bf16)
        return 0

    lax.fori_loop(0, mine, nothing, 0)

    q = zq[mine, :ROWS, :]
    carry, total = block(
        q, col, jnp.zeros((ROWS, 1), f32), jnp.zeros((ROWS, SD), f32), True
    )
    car[...] = jnp.broadcast_to(carry, (ROWS, SD))
    acc[...] = total

    def earlier(k, _):
        c, t = block(zq[mine, :ROWS, :], col - 1 - k, car[:, :1], acc[...], False)
        car[...] = jnp.broadcast_to(c, (ROWS, SD))
        acc[...] = t
        return 0

    lax.fori_loop(0, col, earlier, 0)
    finish(mine, car[:, :1], acc[...])

    def later_rows(z, _):
        q = zq[z, :ROWS, :]
        carry, total = jnp.zeros((ROWS, 1), f32), jnp.zeros((ROWS, SD), f32)
        for y in reversed(range(NY)):
            carry, total = block(q, y, carry, total, False)
        finish(z, carry, total)
        return 0

    lax.fori_loop(mine + 1, NZ, later_rows, 0)


def join_kernel(parts, total, squares):
    rows = []
    run = jnp.zeros((1, ROWS), f32)
    for i in reversed(range(NZ)):
        rows.append(jnp.exp2(-run))
        p = parts[i, ROWS:, :].astype(f32)
        run = run + jnp.concatenate([p[0:1] + p[2:3], p[1:2] + p[3:4]], axis=1)
    factors = jnp.concatenate(rows + [jnp.zeros((SD - NZ, ROWS), f32)], axis=0)
    factors = jnp.transpose(factors)
    out = jnp.zeros((ROWS, SD), f32)
    for k, i in enumerate(reversed(range(NZ))):
        out = out + factors[:, k : k + 1] * parts[i, :ROWS, :].astype(f32)
    total[...] = out
    own = jnp.sum(out * out, axis=1, keepdims=True)
    row = jnp.transpose(jnp.broadcast_to(own, (ROWS, SD)))[:8, :]
    for t in range(8):
        squares[t, :, :] = row


def retain_kernel(lam, tq, inner, entering, gain, out):
    turned = mm(tq[...], slice_order(), ((1,), (1,))).astype(bf16)
    state = jnp.concatenate([entering[y] for y in range(NY)], axis=0)
    steps = (iota((ROWS, RD), 0) + 1).astype(f32)
    value = inner[...] + mm(turned, state) * jnp.exp(lam[0] * steps)
    value = value - jnp.mean(value, axis=1, keepdims=True)
    value = value * lax.rsqrt(jnp.mean(value * value, axis=1, keepdims=True) + epsilon)
    out[...] = (value * gain[...]).astype(bf16)


def output_kernel(total, squares, gain, ret, weights, out):
    mean = jnp.zeros((8, ROWS), f32)
    for t in range(8):
        mean = mean + squares[t]
    scale = lax.rsqrt(mean / STICK_WIDTH + epsilon)
    scale = jnp.concatenate([scale] * (SD // 8), axis=0)
    scale = jnp.transpose(scale)
    stick = (total[...] * scale * gain[...]).astype(bf16)
    both = jnp.concatenate([stick, ret[...]], axis=1)
    for n in range(8):
        cols = slice(n * 256, (n + 1) * 256)
        part = mm(both, weights[cols, :], ((1,), (1,))).astype(bf16)
        for t in range(8):
            out[t % 2, t // 2, :, cols] = part[t * 32 : (t + 1) * 32, :]


def to_all(x, axis):
    return lax.all_to_all(x, axis, 0, 0, tiled=True)


def body(
    inputs,
    input_gain,
    stick_query_w,
    stick_key_w,
    stick_value_w,
    ret_query_w,
    ret_key_w,
    ret_value_w,
    stick_offset,
    ret_log_decay,
    initial_state,
    stick_gain,
    ret_gain,
    stick_out_w,
    ret_out_w,
):
    sds = jax.ShapeDtypeStruct
    z, y, core = lax.axis_index("z"), lax.axis_index("y"), lax.axis_index("c")
    pos = jnp.stack([z, y, core]).astype(jnp.int32)

    shard = jnp.concatenate([stick_out_w, ret_out_w], axis=0).T
    weights = lax.all_gather(shard, SP, axis=0, tiled=True)

    piece = jnp.concatenate(
        [inputs, jnp.broadcast_to(input_gain[None, :], (8, input_gain.shape[0]))], axis=0
    )
    own = to_all(jnp.broadcast_to(piece[None], (4,) + piece.shape), "x")
    other = lax.ppermute(own, "c", [(0, 1), (1, 0)])

    position = ((z * NY + y) * ROWS + jnp.arange(ROWS, dtype=jnp.int32)).astype(f32)
    half = RD // 2
    inverse = rope_base ** (-jnp.arange(half, dtype=f32) / half)
    angles = position[:, None] * inverse[None, :]

    kvs, sq, tq, tk, rv = call(
        project_kernel,
        (
            sds((NY, ROWS + SLICE, RD), bf16),
            sds((ROWS, SD), bf16),
            sds((ROWS, RD), bf16),
            sds((ROWS, RD), bf16),
            sds((ROWS, RD), bf16),
        ),
        [SMEM, SMEM] + [VMEM] * 10,
        1200000000,
    )(
        pos,
        ret_log_decay,
        own,
        other,
        jnp.cos(angles),
        jnp.sin(angles),
        stick_query_w,
        stick_key_w,
        stick_value_w,
        ret_query_w,
        ret_key_w,
        ret_value_w,
    )

    row_kvs = to_all(kvs, "y")
    inner = call(inner_kernel, sds((ROWS, RD), f32), [SMEM] + [VMEM] * 3, 2000000000)(
        ret_log_decay, tq, tk, rv
    )

    first = initial_state.reshape(4, RD)
    first = jnp.concatenate([first[:, :SD], first[:, SD:]], axis=0)
    zq = call(
        totals_kernel, sds((NZ, ROWS + 2 * SLICE + 8, SD), bf16), [SMEM] + [VMEM] * 3, 10000000
    )(ret_log_decay, row_kvs, sq, first)
    col_q = to_all(zq, "z")

    slices = call(
        entering_kernel,
        sds((NY, SLICE, RD), bf16),
        [SMEM, SMEM, VMEM, VMEM],
        10000000,
        [pltpu.VMEM((SLICE, RD), f32)],
    )(pos, ret_log_decay, row_kvs, col_q)
    entering = to_all(slices, "y")

    parts = call(
        stick_kernel,
        sds((NZ, ROWS + 8, SD), bf16),
        [SMEM, SMEM, VMEM, VMEM],
        4000000000,
        [pltpu.VMEM((ROWS, SD), f32), pltpu.VMEM((ROWS, SD), f32), pltpu.VMEM((ROWS, ROWS), bf16)],
    )(pos, stick_offset, row_kvs, col_q)
    parts = to_all(parts, "z")

    total, squares = call(
        join_kernel,
        (sds((ROWS, SD), f32), sds((8, 8, ROWS), f32)),
        [VMEM],
        10000000,
    )(parts)
    squares = to_all(squares, TP)

    ret_normed = call(retain_kernel, sds((ROWS, RD), bf16), [SMEM] + [VMEM] * 4, 100000000)(
        ret_log_decay, tq, inner, entering, ret_gain[None, :]
    )

    out = call(output_kernel, sds((2, 4, 32, D), bf16), [VMEM] * 5, 400000000)(
        total, squares, stick_gain[None, :], ret_normed, weights
    )
    pair = to_all(out, "c").astype(f32).sum(axis=0).astype(bf16)
    layer = to_all(pair, "x").astype(f32).sum(axis=0)
    return layer.astype(bf16)


def solution(mesh):
    split = Mesh(mesh.devices.reshape(NZ, NY, 4, 2), ALL)
    in_specs = (
        P(SP, TP),
        P(TP),
        P(None, TP),
        P(None, TP),
        P(None, TP),
        P(None, TP),
        P(None, TP),
        P(None, TP),
        P(TP),
        P(TP),
        P(TP, SP, None),
        P(TP),
        P(TP),
        P(TP, SP),
        P(TP, SP),
    )
    return jax.shard_map(
        body, mesh=split, in_specs=in_specs, out_specs=P(ALL, None), check_vma=False
    )
```

```python
import functools

import jax
import jax.numpy as jnp
from jax import lax
from jax.experimental import pallas as pl
from jax.experimental.pallas import tpu as pltpu
from jax.sharding import Mesh
from jax.sharding import PartitionSpec as P

D = 2048
STICK_WIDTH = 1024
ROWS = 256
SD = 128
RD = 256
NZ = 8
NY = 8
SLICE = RD // NY
LOG2E = 1.4426950408889634

SP = ("z", "y")
TP = ("x", "c")
ALL = ("z", "y", "x", "c")

epsilon = 1e-06
rope_base = 10000.0
bf16 = jnp.bfloat16
f32 = jnp.float32

VMEM = pl.BlockSpec(memory_space=pltpu.VMEM)
SMEM = pl.BlockSpec(memory_space=pltpu.SMEM)
HBM = pl.BlockSpec(memory_space=pltpu.HBM)


def mm(a, b, dims=((1,), (0,))):
    return lax.dot_general(a, b, (dims, ((), ())), preferred_element_type=f32)


def iota(shape, dim):
    return lax.broadcasted_iota(jnp.int32, shape, dim)


def slice_order():
    r = iota((RD, RD), 0)
    c = iota((RD, RD), 1)
    j, z, k = r // SLICE, (r % SLICE) // 4, r % 4
    return (c == SLICE * z + 4 * j + k).astype(f32).astype(bf16)


def call(kernel, out, in_specs, flops, scratch=()):
    return pl.pallas_call(
        kernel,
        out_shape=out,
        in_specs=in_specs,
        out_specs=jax.tree.map(lambda _: VMEM, out),
        scratch_shapes=list(scratch),
        compiler_params=pltpu.CompilerParams(vmem_limit_bytes=48 * 1024 * 1024),
        cost_estimate=pl.CostEstimate(flops=flops, bytes_accessed=1 << 20, transcendentals=0),
    )


def piece_kernel(inputs, gain, out):
    for x in range(4):
        out[x, :ROWS, :] = inputs[...]
        out[x, ROWS:, :] = jnp.broadcast_to(gain[...], (8, RD))


WIDTHS = (SD, SD, SD, RD, RD, RD)
STARTS = (0, SD, 2 * SD, 3 * SD, 3 * SD + RD, 3 * SD + 2 * RD)
ALL_WIDTH = sum(WIDTHS)


def chunk_copies(part, matrices, buffers, sems):
    return [
        [
            pltpu.make_async_copy(
                w.at[pl.ds(pl.multiple_of((2 * x + part) * RD, RD), RD), :],
                buf.at[x],
                sems.at[x, k],
            )
            for k, (w, buf) in enumerate(zip(matrices, buffers))
        ]
        for x in range(4)
    ]


def projected(copies, feats, buffers, sums, squares):
    for x in range(4):
        raw = feats[x, :ROWS, :].astype(f32)
        gain = feats[x, ROWS : ROWS + 1, :].astype(f32)
        squares = squares + raw * raw
        scaled = (raw * gain).astype(bf16)
        for copy in copies[x]:
            copy.wait()
        for k, buf in enumerate(buffers):
            new = mm(scaled, buf[x])
            sums[k] = new if sums[k] is None else sums[k] + new
    return sums, squares


def first_half_kernel(pos, feats, *refs):
    matrices, (sums, squares), buffers, sems = refs[:6], refs[6:8], refs[8:14], refs[14]
    copies = chunk_copies(pos[2], matrices, buffers, sems)
    for per_chunk in copies:
        for copy in per_chunk:
            copy.start()
    out, square = projected(copies, feats, buffers, [None] * 6, jnp.zeros((ROWS, RD), f32))
    for k in range(6):
        sums[:, STARTS[k] : STARTS[k] + WIDTHS[k]] = out[k]
    squares[...] = square


def second_half_kernel(pos, lam, feats, before, before_squares, cos, sin, columns, *refs):
    matrices, outs, buffers, sems = refs[:6], refs[6:12], refs[12:18], refs[18]
    kv, states, sq, tq, tk, rv = outs
    copies = chunk_copies(1 - pos[2], matrices, buffers, sems)
    for per_chunk in copies:
        for copy in per_chunk:
            copy.start()
    start = [before[:, STARTS[k] : STARTS[k] + WIDTHS[k]] for k in range(6)]
    sums, squares = projected(copies, feats, buffers, start, before_squares[...])
    scale = lax.rsqrt(jnp.sum(squares, axis=1, keepdims=True) / D + epsilon)
    sq_v, sk_v, sv_v, rq_v, rk_v, rv_v = [(s * scale).astype(bf16) for s in sums]
    kv[:, :SD] = sk_v
    kv[:, SD:] = sv_v
    sq[...] = sq_v
    rv[...] = rv_v
    cosine, sine = cos[...], sin[...]
    half = RD // 2

    def turn(v):
        a, b = v[:, :half].astype(f32), v[:, half:].astype(f32)
        return jnp.concatenate([a * cosine - b * sine, b * cosine + a * sine], axis=1)

    tq[...] = turn(rq_v).astype(bf16)
    key = turn(rk_v) * (RD**-0.5)
    tk[...] = key.astype(bf16)
    left = (ROWS - 1 - iota((ROWS, RD), 0)).astype(f32)
    decayed = (key * jnp.exp(lam[0] * left)).astype(bf16)
    state = mm(decayed, rv_v, ((0,), (0,))).astype(bf16)
    ordered = mm(slice_order(), state).astype(bf16)
    for y in range(NY):
        rows = slice(SLICE * y, SLICE * (y + 1))
        states[y, :SLICE, :] = ordered[rows, :SD]
        states[y, SLICE : 2 * SLICE, :] = ordered[rows, SD:]
        states[y, 2 * SLICE :, :] = columns[...]


def inner_kernel(lam, tq, tk, rv, inner):
    gap = (iota((ROWS, ROWS), 0) - iota((ROWS, ROWS), 1)).astype(f32)
    decay = jnp.where(gap >= 0.0, jnp.exp(lam[0] * jnp.maximum(gap, 0.0)), 0.0)
    scores = mm(tq[...], tk[...], ((1,), (1,))) * decay
    inner[...] = mm(scores.astype(bf16), rv[...])


def halves(ref, i, top):
    return jnp.concatenate(
        [ref[i, top : top + SLICE, :], ref[i, top + SLICE : top + 2 * SLICE, :]], axis=1
    ).astype(f32)


def totals_kernel(lam, states, sq, init, out):
    step = jnp.exp(jnp.full((1, RD), lam[0] * ROWS, f32))
    run = jnp.zeros((SLICE, RD), f32)
    for y in range(NY):
        run = run * step + halves(states, y, 0)
    total = run.astype(bf16)
    first = init[...].astype(bf16)
    for z in range(NZ):
        out[z, :ROWS, :] = sq[...]
        out[z, ROWS : ROWS + SLICE, :] = total[:, :SD]
        out[z, ROWS + SLICE : ROWS + 2 * SLICE, :] = total[:, SD:]
        out[z, ROWS + 2 * SLICE :, :] = first


def entering_kernel(pos, lam, states, zq, out, start):
    mine = pos[0]
    step = jnp.exp(jnp.full((1, RD), lam[0] * ROWS, f32))
    row_step = jnp.exp(jnp.full((1, RD), lam[0] * (ROWS * NY), f32))
    top = ROWS + 2 * SLICE
    for z in range(NZ):
        both = zq[z, top : top + 8, :].astype(f32)
        start[4 * z : 4 * z + 4, :SD] = both[:4]
        start[4 * z : 4 * z + 4, SD:] = both[4:]
    before = start[...]
    for z in range(NZ):
        before = jnp.where(z < mine, before * row_step + halves(zq, z, ROWS), before)
    run = before
    for y in range(NY):
        out[y, :, :] = run.astype(bf16)
        run = run * step + halves(states, y, 0)


PAIR = 2
TALL = PAIR * ROWS


def stick_kernel(pos, off, kvs, zq, out, upper, twice, split, acc, car, local, sems):
    copies = [pltpu.make_async_copy(kvs.at[y], local.at[y], sems.at[y]) for y in range(NY)]
    for copy in copies:
        copy.start()
    mine, col = pos[0], pos[1]
    c1 = (SD**-0.5) * LOG2E
    c2 = off[0] * LOG2E
    upper[...] = (iota((ROWS, ROWS), 0) > iota((ROWS, ROWS), 1)).astype(f32).astype(bf16)
    for y in range(NY):
        copies[y].wait()
        twice[y, :, :SD] = local[y, :, :SD]
        twice[y, :, SD:] = local[y, :, :SD]

    def rows_of(c, masked):
        for k in range(PAIR):
            rows = slice(k * ROWS, (k + 1) * ROWS)
            q = zq[c * PAIR + k, :ROWS, :].astype(f32) * c1
            high = q.astype(bf16)
            split[rows, :SD] = high
            split[rows, SD:] = (q - high.astype(f32)).astype(bf16)
        carry = jnp.zeros((TALL, 1), f32)
        total = jnp.zeros((TALL, SD), f32)
        for y in reversed(range(NY)):
            s = mm(split[...], twice[y], ((1,), (1,))) + c2
            soft = jnp.maximum(jnp.log2(1.0 + jnp.exp2(jnp.minimum(s, 126.0))), s)
            power = s - soft
            if masked:
                row = iota((TALL, ROWS), 0)
                row = (row % ROWS) + (row // ROWS) * (NY * ROWS)
                first = ((c * PAIR - mine) * NY + col - y) * ROWS
                allowed = iota((TALL, ROWS), 1) - row < first
                soft = jnp.where(allowed, soft, 0.0)
            rounded = soft.astype(bf16)
            later = mm(rounded, upper[...])
            weight = jnp.exp2(power - (later + carry))
            if masked:
                weight = jnp.where(allowed, weight, 0.0)
            total = total + mm(weight.astype(bf16), local[y, :, SD:])
            carry = carry + (later[:, :1] + rounded[:, :1].astype(f32))
        acc[...] = total
        car[...] = jnp.broadcast_to(carry, (TALL, SD))
        for k in range(PAIR):
            rows = slice(k * ROWS, (k + 1) * ROWS)
            out[c * PAIR + k, :ROWS, :] = acc[rows, :].astype(bf16)
            wide = jnp.transpose(car[rows, :])[:8, :]
            a, b = wide[:, :SD], wide[:, SD:]
            ha, hb = a.astype(bf16).astype(f32), b.astype(bf16).astype(f32)
            row = iota((8, SD), 0)
            low = jnp.where(row == 2, a - ha, jnp.where(row == 3, b - hb, 0.0))
            packed = jnp.where(row == 0, ha, jnp.where(row == 1, hb, low))
            out[c * PAIR + k, ROWS:, :] = packed.astype(bf16)

    own = mine // PAIR

    def nothing(z, _):
        out[z, :, :] = jnp.zeros((ROWS + 8, SD), bf16)
        return 0

    def full(c, _):
        rows_of(c, False)
        return 0

    lax.fori_loop(0, own * PAIR, nothing, 0)
    rows_of(own, True)
    lax.fori_loop(own + 1, NZ // PAIR, full, 0)


def join_kernel(parts, total, squares):
    rows = []
    run = jnp.zeros((1, ROWS), f32)
    for i in reversed(range(NZ)):
        rows.append(jnp.exp2(-run))
        p = parts[i, ROWS:, :].astype(f32)
        run = run + jnp.concatenate([p[0:1] + p[2:3], p[1:2] + p[3:4]], axis=1)
    factors = jnp.concatenate(rows + [jnp.zeros((SD - NZ, ROWS), f32)], axis=0)
    factors = jnp.transpose(factors)
    out = jnp.zeros((ROWS, SD), f32)
    for k, i in enumerate(reversed(range(NZ))):
        out = out + factors[:, k : k + 1] * parts[i, :ROWS, :].astype(f32)
    total[...] = out
    own = jnp.sum(out * out, axis=1, keepdims=True)
    row = jnp.transpose(jnp.broadcast_to(own, (ROWS, SD)))[:8, :]
    for t in range(8):
        squares[t, :, :] = row


def retain_kernel(lam, tq, inner, entering, gain, out):
    turned = mm(tq[...], slice_order(), ((1,), (1,))).astype(bf16)
    state = jnp.concatenate([entering[y] for y in range(NY)], axis=0)
    steps = (iota((ROWS, RD), 0) + 1).astype(f32)
    value = inner[...] + mm(turned, state) * jnp.exp(lam[0] * steps)
    value = value - jnp.mean(value, axis=1, keepdims=True)
    value = value * lax.rsqrt(jnp.mean(value * value, axis=1, keepdims=True) + epsilon)
    out[...] = (value * gain[...]).astype(bf16)


def output_kernel(total, squares, gain, ret, weights, out, local, sems):
    copies = [pltpu.make_async_copy(weights.at[n], local.at[n], sems.at[n]) for n in range(NZ)]
    for copy in copies:
        copy.start()
    mean = jnp.zeros((8, ROWS), f32)
    for t in range(8):
        mean = mean + squares[t]
    scale = lax.rsqrt(mean / STICK_WIDTH + epsilon)
    scale = jnp.concatenate([scale] * (SD // 8), axis=0)
    scale = jnp.transpose(scale)
    stick = (total[...] * scale * gain[...]).astype(bf16)
    both = jnp.concatenate([stick, ret[...]], axis=1)
    for n in range(8):
        cols = slice(n * 256, (n + 1) * 256)
        copies[n].wait()
        block = jnp.concatenate(
            [
                jnp.concatenate([local[n, y, 32 * b : 32 * b + 32, :] for y in range(NY)], axis=0)
                for b in range(3)
            ],
            axis=1,
        )
        part = mm(both, block, ((1,), (1,))).astype(bf16)
        for t in range(8):
            out[t % 2, t // 2, :, cols] = part[t * 32 : (t + 1) * 32, :]


def to_all(x, axis):
    return lax.all_to_all(x, axis, 0, 0, tiled=True)


def body(
    inputs,
    input_gain,
    stick_query_w,
    stick_key_w,
    stick_value_w,
    ret_query_w,
    ret_key_w,
    ret_value_w,
    stick_offset,
    ret_log_decay,
    initial_state,
    stick_gain,
    ret_gain,
    stick_out_w,
    ret_out_w,
):
    sds = jax.ShapeDtypeStruct
    z, y, core = lax.axis_index("z"), lax.axis_index("y"), lax.axis_index("c")
    pos = jnp.stack([z, y, core]).astype(jnp.int32)

    ret_cols = ret_out_w.T
    columns = jnp.concatenate([stick_out_w.T, ret_cols[:, :SD], ret_cols[:, SD:]], axis=0)

    piece = call(piece_kernel, sds((4, ROWS + 8, RD), bf16), [VMEM, VMEM], 1000)(
        inputs, input_gain[None, :]
    )
    own = to_all(piece, "x")
    other = lax.ppermute(own, "c", [(0, 1), (1, 0)])

    position = ((z * NY + y) * ROWS + jnp.arange(ROWS, dtype=jnp.int32)).astype(f32)
    half = RD // 2
    inverse = rope_base ** (-jnp.arange(half, dtype=f32) / half)
    angles = position[:, None] * inverse[None, :]

    matrices = (stick_query_w, stick_key_w, stick_value_w, ret_query_w, ret_key_w, ret_value_w)
    buffers = [pltpu.VMEM((4, RD, w), bf16) for w in WIDTHS] + [pltpu.SemaphoreType.DMA((4, 6))]
    sums, squares = call(
        first_half_kernel,
        (sds((ROWS, ALL_WIDTH), f32), sds((ROWS, RD), f32)),
        [SMEM, VMEM] + [HBM] * 6,
        600000000,
        buffers,
    )(pos, own, *matrices)
    kv, states, sq, tq, tk, rv = call(
        second_half_kernel,
        (
            sds((ROWS, 2 * SD), bf16),
            sds((NY, 2 * SLICE + 96, SD), bf16),
            sds((ROWS, SD), bf16),
            sds((ROWS, RD), bf16),
            sds((ROWS, RD), bf16),
            sds((ROWS, RD), bf16),
        ),
        [SMEM, SMEM] + [VMEM] * 6 + [HBM] * 6,
        600000000,
        buffers,
    )(
        pos,
        ret_log_decay,
        other,
        sums,
        squares,
        jnp.cos(angles),
        jnp.sin(angles),
        columns,
        *matrices,
    )

    row_kv = lax.all_gather(kv, "y", axis=0)
    states = to_all(states, "y")
    weights = lax.all_gather(states[:, 2 * SLICE :, :], "z", axis=0)

    first = initial_state.reshape(4, RD)
    first = jnp.concatenate([first[:, :SD], first[:, SD:]], axis=0)
    zq = call(
        totals_kernel, sds((NZ, ROWS + 2 * SLICE + 8, SD), bf16), [SMEM] + [VMEM] * 3, 10000000
    )(ret_log_decay, states, sq, first)
    col_q = to_all(zq, "z")

    slices = call(
        entering_kernel,
        sds((NY, SLICE, RD), bf16),
        [SMEM, SMEM, VMEM, VMEM],
        10000000,
        [pltpu.VMEM((SLICE, RD), f32)],
    )(pos, ret_log_decay, states, col_q)
    entering = to_all(slices, "y")
    inner = call(inner_kernel, sds((ROWS, RD), f32), [SMEM] + [VMEM] * 3, 2000000000)(
        ret_log_decay, tq, tk, rv
    )

    row_kv, entering = lax.optimization_barrier((row_kv, entering))
    parts = call(
        stick_kernel,
        sds((NZ, ROWS + 8, SD), bf16),
        [SMEM, SMEM, HBM, VMEM],
        4000000000,
        [
            pltpu.VMEM((ROWS, ROWS), bf16),
            pltpu.VMEM((NY, ROWS, 2 * SD), bf16),
            pltpu.VMEM((TALL, 2 * SD), bf16),
            pltpu.VMEM((TALL, SD), f32),
            pltpu.VMEM((TALL, SD), f32),
            pltpu.VMEM((NY, ROWS, 2 * SD), bf16),
            pltpu.SemaphoreType.DMA((NY,)),
        ],
    )(pos, stick_offset, row_kv, col_q)
    parts = to_all(parts, "z")

    total, squares = call(
        join_kernel,
        (sds((ROWS, SD), f32), sds((8, 8, ROWS), f32)),
        [VMEM],
        10000000,
    )(parts)
    squares = to_all(squares, TP)

    ret_normed = call(retain_kernel, sds((ROWS, RD), bf16), [SMEM] + [VMEM] * 4, 100000000)(
        ret_log_decay, tq, inner, entering, ret_gain[None, :]
    )

    out = call(
        output_kernel,
        sds((2, 4, 32, D), bf16),
        [VMEM] * 4 + [HBM],
        400000000,
        [pltpu.VMEM((NZ, NY, 96, SD), bf16), pltpu.SemaphoreType.DMA((NZ,))],
    )(
        total, squares, stick_gain[None, :], ret_normed, weights
    )
    pair = to_all(out, "c").astype(f32).sum(axis=0).astype(bf16)
    layer = to_all(pair, "x").astype(f32).sum(axis=0)
    return layer.astype(bf16)


def solution(mesh):
    split = Mesh(mesh.devices.reshape(NZ, NY, 4, 2), ALL)
    in_specs = (
        P(SP, TP),
        P(TP),
        P(None, TP),
        P(None, TP),
        P(None, TP),
        P(None, TP),
        P(None, TP),
        P(None, TP),
        P(TP),
        P(TP),
        P(TP, SP, None),
        P(TP),
        P(TP),
        P(TP, SP),
        P(TP, SP),
    )
    return jax.shard_map(
        body, mesh=split, in_specs=in_specs, out_specs=P(ALL, None), check_vma=False
    )
```

```python
import functools

import jax
import jax.numpy as jnp
from jax import lax
from jax.experimental import pallas as pl
from jax.experimental.pallas import tpu as pltpu
from jax.sharding import Mesh
from jax.sharding import PartitionSpec as P

D = 2048
STICK_WIDTH = 1024
ROWS = 256
SD = 128
RD = 256
NZ = 8
NY = 8
SLICE = RD // NY
LOG2E = 1.4426950408889634

SP = ("z", "y")
TP = ("x", "c")
ALL = ("z", "y", "x", "c")

epsilon = 1e-06
rope_base = 10000.0
bf16 = jnp.bfloat16
f32 = jnp.float32

WHOLE = 66 * 1000 * 1000

VMEM = pl.BlockSpec(memory_space=pltpu.VMEM)
SMEM = pl.BlockSpec(memory_space=pltpu.SMEM)
HBM = pl.BlockSpec(memory_space=pltpu.HBM)


def mm(a, b, dims=((1,), (0,))):
    return lax.dot_general(a, b, (dims, ((), ())), preferred_element_type=f32)


def iota(shape, dim):
    return lax.broadcasted_iota(jnp.int32, shape, dim)


def slice_order():
    r = iota((RD, RD), 0)
    c = iota((RD, RD), 1)
    j, z, k = r // SLICE, (r % SLICE) // 4, r % 4
    return (c == SLICE * z + 4 * j + k).astype(f32).astype(bf16)


def call(kernel, out, in_specs, flops, scratch=(), limit=48 * 1024 * 1024):
    return pl.pallas_call(
        kernel,
        out_shape=out,
        in_specs=in_specs,
        out_specs=jax.tree.map(lambda _: VMEM, out),
        scratch_shapes=list(scratch),
        compiler_params=pltpu.CompilerParams(vmem_limit_bytes=limit),
        cost_estimate=pl.CostEstimate(flops=flops, bytes_accessed=1 << 20, transcendentals=0),
    )


def piece_kernel(inputs, gain, out):
    for x in range(4):
        out[x, :ROWS, :] = inputs[...]
        out[x, ROWS:, :] = jnp.broadcast_to(gain[...], (8, RD))


WIDTHS = (SD, SD, SD, RD, RD, RD)
STARTS = (0, SD, 2 * SD, 3 * SD, 3 * SD + RD, 3 * SD + 2 * RD)
ALL_WIDTH = sum(WIDTHS)


def project_kernel(pos, lam, own, other, cos, sin, columns, *refs):
    matrices, outs, buf, scaled, sums, sems = refs[:6], refs[6:12], *refs[12:16]
    kv, states, sq, tq, tk, rv = outs
    copies = [
        pltpu.make_async_copy(w, buf.at[:, s : s + n], sems.at[k])
        for k, (w, s, n) in enumerate(zip(matrices, STARTS, WIDTHS))
    ]
    for copy in copies:
        copy.start()
    squares = jnp.zeros((ROWS, RD), f32)
    for part, ref in ((pos[2], own), (1 - pos[2], other)):
        for x in range(4):
            raw = ref[x, :ROWS, :].astype(f32)
            gain = ref[x, ROWS : ROWS + 1, :].astype(f32)
            squares = squares + raw * raw
            col = pl.multiple_of((2 * x + part) * RD, RD)
            scaled[:, pl.ds(col, RD)] = (raw * gain).astype(bf16)
    ready = 0
    for left in range(0, ALL_WIDTH, RD):
        right = min(left + RD, ALL_WIDTH)
        while ready < 6 and STARTS[ready] < right:
            copies[ready].wait()
            ready += 1
        sums[:, left:right] = mm(scaled[...], buf[:, left:right])
    scale = lax.rsqrt(jnp.sum(squares, axis=1, keepdims=True) / D + epsilon)
    sq_v, sk_v, sv_v, rq_v, rk_v, rv_v = [
        (sums[:, s : s + n] * scale).astype(bf16) for s, n in zip(STARTS, WIDTHS)
    ]
    kv[:, :SD] = sk_v
    kv[:, SD:] = sv_v
    sq[...] = sq_v
    rv[...] = rv_v
    cosine, sine = cos[...], sin[...]
    half = RD // 2

    def turn(v):
        a, b = v[:, :half].astype(f32), v[:, half:].astype(f32)
        return jnp.concatenate([a * cosine - b * sine, b * cosine + a * sine], axis=1)

    tq[...] = turn(rq_v).astype(bf16)
    key = turn(rk_v) * (RD**-0.5)
    tk[...] = key.astype(bf16)
    left = (ROWS - 1 - iota((ROWS, RD), 0)).astype(f32)
    decayed = (key * jnp.exp(lam[0] * left)).astype(bf16)
    state = mm(decayed, rv_v, ((0,), (0,))).astype(bf16)
    ordered = mm(slice_order(), state).astype(bf16)
    for y in range(NY):
        rows = slice(SLICE * y, SLICE * (y + 1))
        states[y, :SLICE, :] = ordered[rows, :SD]
        states[y, SLICE : 2 * SLICE, :] = ordered[rows, SD:]
        states[y, 2 * SLICE :, :] = columns[...]


def inner_kernel(lam, tq, tk, rv, inner):
    gap = (iota((ROWS, ROWS), 0) - iota((ROWS, ROWS), 1)).astype(f32)
    decay = jnp.where(gap >= 0.0, jnp.exp(lam[0] * jnp.maximum(gap, 0.0)), 0.0)
    scores = mm(tq[...], tk[...], ((1,), (1,))) * decay
    inner[...] = mm(scores.astype(bf16), rv[...])


def halves(ref, i, top):
    return jnp.concatenate(
        [ref[i, top : top + SLICE, :], ref[i, top + SLICE : top + 2 * SLICE, :]], axis=1
    ).astype(f32)


def totals_kernel(lam, states, sq, init, out):
    step = jnp.exp(jnp.full((1, RD), lam[0] * ROWS, f32))
    run = jnp.zeros((SLICE, RD), f32)
    for y in range(NY):
        run = run * step + halves(states, y, 0)
    total = run.astype(bf16)
    first = init[...].astype(bf16)
    for z in range(NZ):
        out[z, :ROWS, :] = sq[...]
        out[z, ROWS : ROWS + SLICE, :] = total[:, :SD]
        out[z, ROWS + SLICE : ROWS + 2 * SLICE, :] = total[:, SD:]
        out[z, ROWS + 2 * SLICE :, :] = first


def entering_kernel(pos, lam, states, zq, out, start):
    mine = pos[0]
    step = jnp.exp(jnp.full((1, RD), lam[0] * ROWS, f32))
    row_step = jnp.exp(jnp.full((1, RD), lam[0] * (ROWS * NY), f32))
    top = ROWS + 2 * SLICE
    for z in range(NZ):
        both = zq[z, top : top + 8, :].astype(f32)
        start[4 * z : 4 * z + 4, :SD] = both[:4]
        start[4 * z : 4 * z + 4, SD:] = both[4:]
    before = start[...]
    for z in range(NZ):
        before = jnp.where(z < mine, before * row_step + halves(zq, z, ROWS), before)
    run = before
    for y in range(NY):
        out[y, :, :] = run.astype(bf16)
        run = run * step + halves(states, y, 0)


PAIR = 2
TALL = PAIR * ROWS


def stick_kernel(pos, off, kvs, zq, out, upper, twice, split, acc, car, local, sems):
    copies = [pltpu.make_async_copy(kvs.at[y], local.at[y], sems.at[y]) for y in range(NY)]
    for copy in copies:
        copy.start()
    mine, col = pos[0], pos[1]
    c1 = (SD**-0.5) * LOG2E
    c2 = off[0] * LOG2E
    upper[...] = (iota((ROWS, ROWS), 0) > iota((ROWS, ROWS), 1)).astype(f32).astype(bf16)
    for y in range(NY):
        copies[y].wait()
        twice[y, :, :SD] = local[y, :, :SD]
        twice[y, :, SD:] = local[y, :, :SD]

    def rows_of(c, masked):
        for k in range(PAIR):
            rows = slice(k * ROWS, (k + 1) * ROWS)
            q = zq[c * PAIR + k, :ROWS, :].astype(f32) * c1
            high = q.astype(bf16)
            split[rows, :SD] = high
            split[rows, SD:] = (q - high.astype(f32)).astype(bf16)
        carry = jnp.zeros((TALL, 1), f32)
        total = jnp.zeros((TALL, SD), f32)
        for y in reversed(range(NY)):
            s = mm(split[...], twice[y], ((1,), (1,))) + c2
            soft = jnp.maximum(jnp.log2(1.0 + jnp.exp2(jnp.minimum(s, 126.0))), s)
            power = s - soft
            if masked:
                row = iota((TALL, ROWS), 0)
                row = (row % ROWS) + (row // ROWS) * (NY * ROWS)
                first = ((c * PAIR - mine) * NY + col - y) * ROWS
                allowed = iota((TALL, ROWS), 1) - row < first
                soft = jnp.where(allowed, soft, 0.0)
            rounded = soft.astype(bf16)
            later = mm(rounded, upper[...])
            weight = jnp.exp2(power - (later + carry))
            if masked:
                weight = jnp.where(allowed, weight, 0.0)
            total = total + mm(weight.astype(bf16), local[y, :, SD:])
            carry = carry + (later[:, :1] + rounded[:, :1].astype(f32))
        acc[...] = total
        car[...] = jnp.broadcast_to(carry, (TALL, SD))
        for k in range(PAIR):
            rows = slice(k * ROWS, (k + 1) * ROWS)
            out[c * PAIR + k, :ROWS, :] = acc[rows, :].astype(bf16)
            wide = jnp.transpose(car[rows, :])[:8, :]
            a, b = wide[:, :SD], wide[:, SD:]
            ha, hb = a.astype(bf16).astype(f32), b.astype(bf16).astype(f32)
            row = iota((8, SD), 0)
            low = jnp.where(row == 2, a - ha, jnp.where(row == 3, b - hb, 0.0))
            packed = jnp.where(row == 0, ha, jnp.where(row == 1, hb, low))
            out[c * PAIR + k, ROWS:, :] = packed.astype(bf16)

    own = mine // PAIR

    def nothing(z, _):
        out[z, :, :] = jnp.zeros((ROWS + 8, SD), bf16)
        return 0

    def full(c, _):
        rows_of(c, False)
        return 0

    lax.fori_loop(0, own * PAIR, nothing, 0)
    rows_of(own, True)
    lax.fori_loop(own + 1, NZ // PAIR, full, 0)


def join_kernel(parts, total, squares):
    rows = []
    run = jnp.zeros((1, ROWS), f32)
    for i in reversed(range(NZ)):
        rows.append(jnp.exp2(-run))
        p = parts[i, ROWS:, :].astype(f32)
        run = run + jnp.concatenate([p[0:1] + p[2:3], p[1:2] + p[3:4]], axis=1)
    factors = jnp.concatenate(rows + [jnp.zeros((SD - NZ, ROWS), f32)], axis=0)
    factors = jnp.transpose(factors)
    out = jnp.zeros((ROWS, SD), f32)
    for k, i in enumerate(reversed(range(NZ))):
        out = out + factors[:, k : k + 1] * parts[i, :ROWS, :].astype(f32)
    total[...] = out
    own = jnp.sum(out * out, axis=1, keepdims=True)
    row = jnp.transpose(jnp.broadcast_to(own, (ROWS, SD)))[:8, :]
    for t in range(8):
        squares[t, :, :] = row


def retain_kernel(lam, tq, inner, entering, gain, out):
    turned = mm(tq[...], slice_order(), ((1,), (1,))).astype(bf16)
    state = jnp.concatenate([entering[y] for y in range(NY)], axis=0)
    steps = (iota((ROWS, RD), 0) + 1).astype(f32)
    value = inner[...] + mm(turned, state) * jnp.exp(lam[0] * steps)
    value = value - jnp.mean(value, axis=1, keepdims=True)
    value = value * lax.rsqrt(jnp.mean(value * value, axis=1, keepdims=True) + epsilon)
    out[...] = (value * gain[...]).astype(bf16)


def output_kernel(total, squares, gain, ret, weights, out, local, sems):
    copies = [pltpu.make_async_copy(weights.at[n], local.at[n], sems.at[n]) for n in range(NZ)]
    for copy in copies:
        copy.start()
    mean = jnp.zeros((8, ROWS), f32)
    for t in range(8):
        mean = mean + squares[t]
    scale = lax.rsqrt(mean / STICK_WIDTH + epsilon)
    scale = jnp.concatenate([scale] * (SD // 8), axis=0)
    scale = jnp.transpose(scale)
    stick = (total[...] * scale * gain[...]).astype(bf16)
    both = jnp.concatenate([stick, ret[...]], axis=1)
    for n in range(8):
        cols = slice(n * 256, (n + 1) * 256)
        copies[n].wait()
        block = jnp.concatenate(
            [
                jnp.concatenate([local[n, y, 32 * b : 32 * b + 32, :] for y in range(NY)], axis=0)
                for b in range(3)
            ],
            axis=1,
        )
        part = mm(both, block, ((1,), (1,))).astype(bf16)
        for t in range(8):
            out[t % 2, t // 2, :, cols] = part[t * 32 : (t + 1) * 32, :]


def to_all(x, axis):
    return lax.all_to_all(x, axis, 0, 0, tiled=True)


def body(
    inputs,
    input_gain,
    stick_query_w,
    stick_key_w,
    stick_value_w,
    ret_query_w,
    ret_key_w,
    ret_value_w,
    stick_offset,
    ret_log_decay,
    initial_state,
    stick_gain,
    ret_gain,
    stick_out_w,
    ret_out_w,
):
    sds = jax.ShapeDtypeStruct
    z, y, core = lax.axis_index("z"), lax.axis_index("y"), lax.axis_index("c")
    pos = jnp.stack([z, y, core]).astype(jnp.int32)

    ret_cols = ret_out_w.T
    columns = jnp.concatenate([stick_out_w.T, ret_cols[:, :SD], ret_cols[:, SD:]], axis=0)

    piece = call(piece_kernel, sds((4, ROWS + 8, RD), bf16), [VMEM, VMEM], 1000, (), WHOLE)(
        inputs, input_gain[None, :]
    )
    own = to_all(piece, "x")
    other = lax.ppermute(own, "c", [(0, 1), (1, 0)])

    position = ((z * NY + y) * ROWS + jnp.arange(ROWS, dtype=jnp.int32)).astype(f32)
    half = RD // 2
    inverse = rope_base ** (-jnp.arange(half, dtype=f32) / half)
    angles = position[:, None] * inverse[None, :]

    matrices = (stick_query_w, stick_key_w, stick_value_w, ret_query_w, ret_key_w, ret_value_w)
    kv, states, sq, tq, tk, rv = call(
        project_kernel,
        (
            sds((ROWS, 2 * SD), bf16),
            sds((NY, 2 * SLICE + 96, SD), bf16),
            sds((ROWS, SD), bf16),
            sds((ROWS, RD), bf16),
            sds((ROWS, RD), bf16),
            sds((ROWS, RD), bf16),
        ),
        [SMEM, SMEM] + [VMEM] * 5 + [HBM] * 6,
        1200000000,
        [
            pltpu.VMEM((D, ALL_WIDTH), bf16),
            pltpu.VMEM((ROWS, D), bf16),
            pltpu.VMEM((ROWS, ALL_WIDTH), f32),
            pltpu.SemaphoreType.DMA((6,)),
        ],
        WHOLE,
    )(
        pos,
        ret_log_decay,
        own,
        other,
        jnp.cos(angles),
        jnp.sin(angles),
        columns,
        *matrices,
    )

    row_kv = lax.all_gather(kv, "y", axis=0)
    states = to_all(states, "y")
    weights = lax.all_gather(states[:, 2 * SLICE :, :], "z", axis=0)

    first = initial_state.reshape(4, RD)
    first = jnp.concatenate([first[:, :SD], first[:, SD:]], axis=0)
    zq = call(
        totals_kernel, sds((NZ, ROWS + 2 * SLICE + 8, SD), bf16), [SMEM] + [VMEM] * 3, 10000000
    )(ret_log_decay, states, sq, first)
    col_q = to_all(zq, "z")

    slices = call(
        entering_kernel,
        sds((NY, SLICE, RD), bf16),
        [SMEM, SMEM, VMEM, VMEM],
        10000000,
        [pltpu.VMEM((SLICE, RD), f32)],
    )(pos, ret_log_decay, states, col_q)
    entering = to_all(slices, "y")
    inner = call(inner_kernel, sds((ROWS, RD), f32), [SMEM] + [VMEM] * 3, 2000000000)(
        ret_log_decay, tq, tk, rv
    )

    row_kv, entering = lax.optimization_barrier((row_kv, entering))
    parts = call(
        stick_kernel,
        sds((NZ, ROWS + 8, SD), bf16),
        [SMEM, SMEM, HBM, VMEM],
        4000000000,
        [
            pltpu.VMEM((ROWS, ROWS), bf16),
            pltpu.VMEM((NY, ROWS, 2 * SD), bf16),
            pltpu.VMEM((TALL, 2 * SD), bf16),
            pltpu.VMEM((TALL, SD), f32),
            pltpu.VMEM((TALL, SD), f32),
            pltpu.VMEM((NY, ROWS, 2 * SD), bf16),
            pltpu.SemaphoreType.DMA((NY,)),
        ],
        WHOLE,
    )(pos, stick_offset, row_kv, col_q)
    parts = to_all(parts, "z")

    total, squares = call(
        join_kernel,
        (sds((ROWS, SD), f32), sds((8, 8, ROWS), f32)),
        [VMEM],
        10000000,
    )(parts)
    squares = to_all(squares, TP)

    ret_normed = call(retain_kernel, sds((ROWS, RD), bf16), [SMEM] + [VMEM] * 4, 100000000)(
        ret_log_decay, tq, inner, entering, ret_gain[None, :]
    )

    out = call(
        output_kernel,
        sds((2, 4, 32, D), bf16),
        [VMEM] * 4 + [HBM],
        400000000,
        [pltpu.VMEM((NZ, NY, 96, SD), bf16), pltpu.SemaphoreType.DMA((NZ,))],
        WHOLE,
    )(
        total, squares, stick_gain[None, :], ret_normed, weights
    )
    pair = to_all(out, "c").astype(f32).sum(axis=0).astype(bf16)
    layer = to_all(pair, "x").astype(f32).sum(axis=0)
    return layer.astype(bf16)


def solution(mesh):
    split = Mesh(mesh.devices.reshape(NZ, NY, 4, 2), ALL)
    in_specs = (
        P(SP, TP),
        P(TP),
        P(None, TP),
        P(None, TP),
        P(None, TP),
        P(None, TP),
        P(None, TP),
        P(None, TP),
        P(TP),
        P(TP),
        P(TP, SP, None),
        P(TP),
        P(TP),
        P(TP, SP),
        P(TP, SP),
    )
    return jax.shard_map(
        body, mesh=split, in_specs=in_specs, out_specs=P(ALL, None), check_vma=False
    )
```

```python
import jax
import jax.numpy as jnp
from jax import lax
from jax.experimental import pallas as pl
from jax.experimental.pallas import tpu as pltpu
from jax.sharding import Mesh
from jax.sharding import PartitionSpec as P


D = 2048
STICK_WIDTH = 1024
ROWS = 256
SD = 128
RD = 256
NZ = 8
NY = 8
LOG2E = 1.4426950408889634

SP = ("z", "y")
TP = ("x", "c")
ALL = ("z", "y", "x", "c")

epsilon = 1e-06
rope_base = 10000.0
bf16 = jnp.bfloat16
f32 = jnp.float32

WHOLE = 66 * 1000 * 1000

VMEM = pl.BlockSpec(memory_space=pltpu.VMEM)
SMEM = pl.BlockSpec(memory_space=pltpu.SMEM)
HBM = pl.BlockSpec(memory_space=pltpu.HBM)


def mm(a, b, dims=((1,), (0,))):
    return lax.dot_general(a, b, (dims, ((), ())), preferred_element_type=f32)


def iota(shape, dim):
    return lax.broadcasted_iota(jnp.int32, shape, dim)


def spread(h):
    r = iota((2 * RD, RD), 0)
    return ((r // 8 * 4 + r % 4 == iota((2 * RD, RD), 1)) & (r // 4 % 2 == h)).astype(f32).astype(bf16)


def call(kernel, out, in_specs, flops, scratch=(), limit=48 * 1024 * 1024):
    return pl.pallas_call(
        kernel,
        out_shape=out,
        in_specs=in_specs,
        out_specs=jax.tree.map(lambda _: VMEM, out),
        scratch_shapes=list(scratch),
        compiler_params=pltpu.CompilerParams(vmem_limit_bytes=limit),
        cost_estimate=pl.CostEstimate(flops=flops, bytes_accessed=1 << 20, transcendentals=0),
    )


def piece_kernel(inputs, gain, out):
    for x in range(4):
        out[x, :ROWS, :] = inputs[...]
        out[x, ROWS:, :] = jnp.broadcast_to(gain[...], (8, RD))


def three_products(pos, own, other, matrices, buf, scaled, sums, sems):
    width = buf.shape[1] // 3
    copies = [
        pltpu.make_async_copy(w, buf.at[:, k * width : (k + 1) * width], sems.at[k])
        for k, w in enumerate(matrices)
    ]
    for copy in copies:
        copy.start()
    squares = jnp.zeros((ROWS, RD), f32)
    for part, ref in ((pos[2], own), (1 - pos[2], other)):
        for x in range(4):
            raw = ref[x, :ROWS, :].astype(f32)
            gain = ref[x, ROWS : ROWS + 1, :].astype(f32)
            squares = squares + raw * raw
            col = pl.multiple_of((2 * x + part) * RD, RD)
            scaled[:, pl.ds(col, RD)] = (raw * gain).astype(bf16)
    ready = 0
    for left in range(0, 3 * width, RD):
        right = min(left + RD, 3 * width)
        while ready < 3 and ready * width < right:
            copies[ready].wait()
            ready += 1
        sums[:, left:right] = mm(scaled[...], buf[:, left:right])
    scale = lax.rsqrt(jnp.sum(squares, axis=1, keepdims=True) / D + epsilon)
    return [(sums[:, k * width : (k + 1) * width] * scale).astype(bf16) for k in range(3)]


def stick_project_kernel(pos, own, other, columns, wq, wk, wv, kv, queries, *work):
    query, key, value = three_products(pos, own, other, (wq, wk, wv), *work)
    kv[:, :SD] = key
    kv[:, SD:] = value
    for z in range(NZ):
        queries[z, :ROWS, :] = query
        queries[z, ROWS:, :] = columns[...]


def ret_project_kernel(
    pos, lam, own, other, cos, sin, wq, wk, wv, states, tq, tk, rv, *work
):
    query, key, value = three_products(pos, own, other, (wq, wk, wv), *work)
    rv[...] = value
    cosine, sine = cos[...], sin[...]
    half = RD // 2

    def turn(v):
        a, b = v[:, :half].astype(f32), v[:, half:].astype(f32)
        return jnp.concatenate([a * cosine - b * sine, b * cosine + a * sine], axis=1)

    tq[...] = turn(query).astype(bf16)
    key = turn(key) * (RD**-0.5)
    tk[...] = key.astype(bf16)
    left = (ROWS - 1 - iota((ROWS, RD), 0)).astype(f32)
    decayed = (key * jnp.exp(lam[0] * left)).astype(bf16)
    state = mm(decayed, value, ((0,), (0,))).astype(bf16)
    slices = mm(spread(0), state[:, :SD]) + mm(spread(1), state[:, SD:])
    states[...] = slices.astype(bf16).reshape(NZ * NY, 8, SD)


def inner_kernel(lam, tq, tk, rv, inner):
    gap = (iota((ROWS, ROWS), 0) - iota((ROWS, ROWS), 1)).astype(f32)
    decay = jnp.where(gap >= 0.0, jnp.exp(lam[0] * jnp.maximum(gap, 0.0)), 0.0)
    scores = mm(tq[...], tk[...], ((1,), (1,))) * decay
    inner[...] = mm(scores.astype(bf16), rv[...])


def scan_kernel(lam, states, first, out):
    step = jnp.exp(jnp.full((8, SD), lam[0] * ROWS, f32))
    run = first[...]
    for b in range(NZ * NY):
        out[b, :, :] = run.astype(bf16)
        run = run * step + states[b].astype(f32)


PAIR = 2
TALL = PAIR * ROWS


def stick_kernel(pos, off, kvs, zq, out, upper, twice, split, acc, car, local, sems):
    copies = [pltpu.make_async_copy(kvs.at[y], local.at[y], sems.at[y]) for y in range(NY)]
    for copy in copies:
        copy.start()
    mine, col = pos[0], pos[1]
    c1 = (SD**-0.5) * LOG2E
    c2 = off[0] * LOG2E
    upper[...] = (iota((ROWS, ROWS), 0) > iota((ROWS, ROWS), 1)).astype(f32).astype(bf16)
    for y in range(NY):
        copies[y].wait()
        twice[y, :, :SD] = local[y, :, :SD]
        twice[y, :, SD:] = local[y, :, :SD]

    def rows_of(c, masked):
        for k in range(PAIR):
            rows = slice(k * ROWS, (k + 1) * ROWS)
            q = zq[c * PAIR + k, :ROWS, :].astype(f32) * c1
            high = q.astype(bf16)
            split[rows, :SD] = high
            split[rows, SD:] = (q - high.astype(f32)).astype(bf16)
        carry = jnp.zeros((TALL, 1), f32)
        total = jnp.zeros((TALL, SD), f32)
        for y in reversed(range(NY)):
            s = mm(split[...], twice[y], ((1,), (1,))) + c2
            soft = jnp.maximum(jnp.log2(1.0 + jnp.exp2(jnp.minimum(s, 126.0))), s)
            power = s - soft
            if masked:
                row = iota((TALL, ROWS), 0)
                row = (row % ROWS) + (row // ROWS) * (NY * ROWS)
                first = ((c * PAIR - mine) * NY + col - y) * ROWS
                allowed = iota((TALL, ROWS), 1) - row < first
                soft = jnp.where(allowed, soft, 0.0)
            rounded = soft.astype(bf16)
            later = mm(rounded, upper[...])
            weight = jnp.exp2(power - (later + carry))
            if masked:
                weight = jnp.where(allowed, weight, 0.0)
            total = total + mm(weight.astype(bf16), local[y, :, SD:])
            carry = carry + (later[:, :1] + rounded[:, :1].astype(f32))
        acc[...] = total
        car[...] = jnp.broadcast_to(carry, (TALL, SD))
        for k in range(PAIR):
            rows = slice(k * ROWS, (k + 1) * ROWS)
            out[c * PAIR + k, :ROWS, :] = acc[rows, :].astype(bf16)
            wide = jnp.transpose(car[rows, :])[:8, :]
            a, b = wide[:, :SD], wide[:, SD:]
            ha, hb = a.astype(bf16).astype(f32), b.astype(bf16).astype(f32)
            row = iota((8, SD), 0)
            low = jnp.where(row == 2, a - ha, jnp.where(row == 3, b - hb, 0.0))
            packed = jnp.where(row == 0, ha, jnp.where(row == 1, hb, low))
            out[c * PAIR + k, ROWS:, :] = packed.astype(bf16)

    own = mine // PAIR

    def nothing(z, _):
        out[z, :, :] = jnp.zeros((ROWS + 8, SD), bf16)
        return 0

    def full(c, _):
        rows_of(c, False)
        return 0

    lax.fori_loop(0, own * PAIR, nothing, 0)
    rows_of(own, True)
    lax.fori_loop(own + 1, NZ // PAIR, full, 0)


def join_kernel(parts, total, squares):
    rows = []
    run = jnp.zeros((1, ROWS), f32)
    for i in reversed(range(NZ)):
        rows.append(jnp.exp2(-run))
        p = parts[i, ROWS:, :].astype(f32)
        run = run + jnp.concatenate([p[0:1] + p[2:3], p[1:2] + p[3:4]], axis=1)
    factors = jnp.concatenate(rows + [jnp.zeros((SD - NZ, ROWS), f32)], axis=0)
    factors = jnp.transpose(factors)
    out = jnp.zeros((ROWS, SD), f32)
    for k, i in enumerate(reversed(range(NZ))):
        out = out + factors[:, k : k + 1] * parts[i, :ROWS, :].astype(f32)
    total[...] = out
    own = jnp.sum(out * out, axis=1, keepdims=True)
    row = jnp.transpose(jnp.broadcast_to(own, (ROWS, SD)))[:8, :]
    for t in range(8):
        squares[t, :, :] = row


def retain_kernel(lam, tq, inner, entering, gain, out):
    slices = entering[...].reshape(2 * RD, SD)
    state = [mm(spread(h), slices, ((0,), (0,))).astype(bf16) for h in range(2)]
    state = jnp.concatenate(state, axis=1)
    steps = (iota((ROWS, RD), 0) + 1).astype(f32)
    value = inner[...] + mm(tq[...], state) * jnp.exp(lam[0] * steps)
    value = value - jnp.mean(value, axis=1, keepdims=True)
    value = value * lax.rsqrt(jnp.mean(value * value, axis=1, keepdims=True) + epsilon)
    out[...] = (value * gain[...]).astype(bf16)


def output_kernel(total, squares, gain, ret, weights, out):
    mean = jnp.zeros((8, ROWS), f32)
    for t in range(8):
        mean = mean + squares[t]
    scale = lax.rsqrt(mean / STICK_WIDTH + epsilon)
    scale = jnp.concatenate([scale] * (SD // 8), axis=0)
    scale = jnp.transpose(scale)
    stick = (total[...] * scale * gain[...]).astype(bf16)
    both = jnp.concatenate([stick, ret[...]], axis=1)
    for n in range(8):
        cols = slice(n * 256, (n + 1) * 256)
        block = jnp.concatenate(
            [
                jnp.concatenate([weights[y, n, 32 * b : 32 * b + 32, :] for y in range(NY)], axis=0)
                for b in range(3)
            ],
            axis=1,
        )
        part = mm(both, block, ((1,), (1,))).astype(bf16)
        for t in range(8):
            out[t % 2, t // 2, :, cols] = part[t * 32 : (t + 1) * 32, :]


def to_all(x, axis):
    return lax.all_to_all(x, axis, 0, 0, tiled=True)


def body(
    inputs,
    input_gain,
    stick_query_w,
    stick_key_w,
    stick_value_w,
    ret_query_w,
    ret_key_w,
    ret_value_w,
    stick_offset,
    ret_log_decay,
    initial_state,
    stick_gain,
    ret_gain,
    stick_out_w,
    ret_out_w,
):
    sds = jax.ShapeDtypeStruct
    z, y, core = lax.axis_index("z"), lax.axis_index("y"), lax.axis_index("c")
    pos = jnp.stack([z, y, core]).astype(jnp.int32)

    ret_cols = ret_out_w.T
    columns = jnp.concatenate([stick_out_w.T, ret_cols[:, :SD], ret_cols[:, SD:]], axis=0)

    piece = call(piece_kernel, sds((4, ROWS + 8, RD), bf16), [VMEM, VMEM], 1000, (), WHOLE)(
        inputs, input_gain[None, :]
    )
    own = to_all(piece, "x")
    other = lax.ppermute(own, "c", [(0, 1), (1, 0)])

    position = ((z * NY + y) * ROWS + jnp.arange(ROWS, dtype=jnp.int32)).astype(f32)
    half = RD // 2
    inverse = rope_base ** (-jnp.arange(half, dtype=f32) / half)
    angles = position[:, None] * inverse[None, :]

    def work(width):
        return [
            pltpu.VMEM((D, 3 * width), bf16),
            pltpu.VMEM((ROWS, D), bf16),
            pltpu.VMEM((ROWS, 3 * width), f32),
            pltpu.SemaphoreType.DMA((3,)),
        ]

    kv, queries = call(
        stick_project_kernel,
        (sds((ROWS, 2 * SD), bf16), sds((NZ, ROWS + 96, SD), bf16)),
        [SMEM] + [VMEM] * 3 + [HBM] * 3,
        400000000,
        work(SD),
        WHOLE,
    )(pos, own, other, columns, stick_query_w, stick_key_w, stick_value_w)
    ret_project = call(
        ret_project_kernel,
        (sds((NZ * NY, 8, SD), bf16),) + (sds((ROWS, RD), bf16),) * 3,
        [SMEM, SMEM] + [VMEM] * 4 + [HBM] * 3,
        6000000000,
        work(RD),
        WHOLE,
    )
    cosine, sine = jnp.cos(angles), jnp.sin(angles)
    states, tq, tk, rv = ret_project(
        pos,
        ret_log_decay,
        own,
        other,
        cosine,
        sine,
        ret_query_w,
        ret_key_w,
        ret_value_w,
    )

    row_kv = lax.all_gather(kv, "y", axis=0)
    col_q = to_all(queries, "z")
    weights = lax.all_gather(col_q[:, ROWS:, :], "y", axis=0)

    first = initial_state.reshape(4, RD)
    first = jnp.concatenate([first[:, :SD], first[:, SD:]], axis=0)
    slices = call(scan_kernel, sds((NZ * NY, 8, SD), bf16), [SMEM, VMEM, VMEM], 1000000)(
        ret_log_decay, to_all(states, SP), first
    )
    entering = to_all(slices, SP)
    inner = call(inner_kernel, sds((ROWS, RD), f32), [SMEM] + [VMEM] * 3, 2000000000)(
        ret_log_decay, tq, tk, rv
    )

    row_kv, entering = lax.optimization_barrier((row_kv, entering))
    parts = call(
        stick_kernel,
        sds((NZ, ROWS + 8, SD), bf16),
        [SMEM, SMEM, HBM, VMEM],
        4000000000,
        [
            pltpu.VMEM((ROWS, ROWS), bf16),
            pltpu.VMEM((NY, ROWS, 2 * SD), bf16),
            pltpu.VMEM((TALL, 2 * SD), bf16),
            pltpu.VMEM((TALL, SD), f32),
            pltpu.VMEM((TALL, SD), f32),
            pltpu.VMEM((NY, ROWS, 2 * SD), bf16),
            pltpu.SemaphoreType.DMA((NY,)),
        ],
        WHOLE,
    )(pos, stick_offset, row_kv, col_q)
    parts = to_all(parts, "z")

    total, squares = call(
        join_kernel,
        (sds((ROWS, SD), f32), sds((8, 8, ROWS), f32)),
        [VMEM],
        10000000,
    )(parts)
    squares = to_all(squares, TP)

    ret_normed = call(retain_kernel, sds((ROWS, RD), bf16), [SMEM] + [VMEM] * 4, 100000000)(
        ret_log_decay, tq, inner, entering, ret_gain[None, :]
    )

    out = call(
        output_kernel,
        sds((2, 4, 32, D), bf16),
        [VMEM] * 5,
        400000000,
    )(
        total, squares, stick_gain[None, :], ret_normed, weights
    )
    pair = to_all(out, "c").astype(f32).sum(axis=0).astype(bf16)
    layer = to_all(pair, "x").astype(f32).sum(axis=0)
    return layer.astype(bf16)


def solution(mesh):
    split = Mesh(mesh.devices.reshape(NZ, NY, 4, 2), ALL)
    in_specs = (
        P(SP, TP),
        P(TP),
        P(None, TP),
        P(None, TP),
        P(None, TP),
        P(None, TP),
        P(None, TP),
        P(None, TP),
        P(TP),
        P(TP),
        P(TP, SP, None),
        P(TP),
        P(TP),
        P(TP, SP),
        P(TP, SP),
    )
    return jax.shard_map(
        body, mesh=split, in_specs=in_specs, out_specs=P(ALL, None), check_vma=False
    )
```

```python
import jax
import jax.numpy as jnp
from jax import lax
from jax.experimental import pallas as pl
from jax.experimental.pallas import tpu as pltpu
from jax.sharding import Mesh
from jax.sharding import PartitionSpec as P


D = 2048
STICK_WIDTH = 1024
ROWS = 256
SD = 128
RD = 256
NZ = 8
NY = 8
LOG2E = 1.4426950408889634

SP = ("z", "y")
TP = ("x", "c")
ALL = ("z", "y", "x", "c")

epsilon = 1e-06
rope_base = 10000.0
bf16 = jnp.bfloat16
f32 = jnp.float32

WHOLE = 66 * 1000 * 1000

VMEM = pl.BlockSpec(memory_space=pltpu.VMEM)
SMEM = pl.BlockSpec(memory_space=pltpu.SMEM)
HBM = pl.BlockSpec(memory_space=pltpu.HBM)


def mm(a, b, dims=((1,), (0,))):
    return lax.dot_general(a, b, (dims, ((), ())), preferred_element_type=f32)


def iota(shape, dim):
    return lax.broadcasted_iota(jnp.int32, shape, dim)


def spread(h):
    r = iota((2 * RD, RD), 0)
    return ((r // 8 * 4 + r % 4 == iota((2 * RD, RD), 1)) & (r // 4 % 2 == h)).astype(f32).astype(bf16)


def call(kernel, out, in_specs, flops, scratch=(), limit=48 * 1024 * 1024):
    return pl.pallas_call(
        kernel,
        out_shape=out,
        in_specs=in_specs,
        out_specs=jax.tree.map(lambda _: VMEM, out),
        scratch_shapes=list(scratch),
        compiler_params=pltpu.CompilerParams(vmem_limit_bytes=limit),
        cost_estimate=pl.CostEstimate(flops=flops, bytes_accessed=1 << 20, transcendentals=0),
    )


def piece_kernel(inputs, gain, out):
    for x in range(4):
        out[x, :ROWS, :] = inputs[...]
        out[x, ROWS:, :] = jnp.broadcast_to(gain[...][None, :], (8, RD))


def three_products(pos, own, other, matrices, buf, scaled, sums, sems):
    width = buf.shape[1] // 3
    copies = [
        pltpu.make_async_copy(w, buf.at[:, k * width : (k + 1) * width], sems.at[k])
        for k, w in enumerate(matrices)
    ]
    for copy in copies:
        copy.start()
    squares = jnp.zeros((ROWS, RD), f32)
    for part, ref in ((pos[2], own), (1 - pos[2], other)):
        for x in range(4):
            raw = ref[x, :ROWS, :].astype(f32)
            gain = ref[x, ROWS : ROWS + 1, :].astype(f32)
            squares = squares + raw * raw
            col = pl.multiple_of((2 * x + part) * RD, RD)
            scaled[:, pl.ds(col, RD)] = (raw * gain).astype(bf16)
    ready = 0
    for left in range(0, 3 * width, RD):
        right = min(left + RD, 3 * width)
        while ready < 3 and ready * width < right:
            copies[ready].wait()
            ready += 1
        sums[:, left:right] = mm(scaled[...], buf[:, left:right])
    scale = lax.rsqrt(jnp.sum(squares, axis=1, keepdims=True) / D + epsilon)
    return [(sums[:, k * width : (k + 1) * width] * scale).astype(bf16) for k in range(3)]


def stick_project_kernel(pos, own, other, columns, wq, wk, wv, kv, queries, *work):
    query, key, value = three_products(pos, own, other, (wq, wk, wv), *work)
    kv[:, :SD] = key
    kv[:, SD:] = value
    for z in range(NZ):
        queries[z, :ROWS, :] = query
        queries[z, ROWS:, :] = columns[...]


def ret_project_kernel(
    pos, lam, own, other, cos, sin, wq, wk, wv, states, tq, tk, rv, *work
):
    query, key, value = three_products(pos, own, other, (wq, wk, wv), *work)
    rv[...] = value
    cosine, sine = cos[...], sin[...]
    half = RD // 2

    def turn(v):
        a, b = v[:, :half].astype(f32), v[:, half:].astype(f32)
        return jnp.concatenate([a * cosine - b * sine, b * cosine + a * sine], axis=1)

    tq[...] = turn(query).astype(bf16)
    key = turn(key) * (RD**-0.5)
    tk[...] = key.astype(bf16)
    left = (ROWS - 1 - iota((ROWS, RD), 0)).astype(f32)
    decayed = (key * jnp.exp(lam[0] * left)).astype(bf16)
    state = mm(decayed, value, ((0,), (0,))).astype(bf16)
    slices = mm(spread(0), state[:, :SD]) + mm(spread(1), state[:, SD:])
    states[...] = slices.astype(bf16).reshape(NZ * NY, 8, SD)


def inner_kernel(lam, tq, tk, rv, inner):
    gap = (iota((ROWS, ROWS), 0) - iota((ROWS, ROWS), 1)).astype(f32)
    decay = jnp.where(gap >= 0.0, jnp.exp(lam[0] * jnp.maximum(gap, 0.0)), 0.0)
    scores = mm(tq[...], tk[...], ((1,), (1,))) * decay
    inner[...] = mm(scores.astype(bf16), rv[...])


def scan_kernel(lam, states, first, out):
    step = jnp.exp(jnp.full((8, SD), lam[0] * ROWS, f32))
    run = first[...]
    for b in range(NZ * NY):
        out[b, :, :] = run.astype(bf16)
        run = run * step + states[b].astype(f32)


PAIR = 2
TALL = PAIR * ROWS


def stick_kernel(pos, off, kvs, zq, out, upper, twice, split, acc, car, local, sems):
    copies = [pltpu.make_async_copy(kvs.at[y], local.at[y], sems.at[y]) for y in range(NY)]
    for copy in copies:
        copy.start()
    mine, col = pos[0], pos[1]
    c1 = (SD**-0.5) * LOG2E
    c2 = off[0] * LOG2E
    upper[...] = (iota((ROWS, ROWS), 0) > iota((ROWS, ROWS), 1)).astype(f32).astype(bf16)
    for y in range(NY):
        copies[y].wait()
        twice[y, :, :SD] = local[y, :, :SD]
        twice[y, :, SD:] = local[y, :, :SD]

    def rows_of(c, masked):
        for k in range(PAIR):
            rows = slice(k * ROWS, (k + 1) * ROWS)
            q = zq[c * PAIR + k, :ROWS, :].astype(f32) * c1
            high = q.astype(bf16)
            split[rows, :SD] = high
            split[rows, SD:] = (q - high.astype(f32)).astype(bf16)
        carry = jnp.zeros((TALL, 1), f32)
        total = jnp.zeros((TALL, SD), f32)
        for y in reversed(range(NY)):
            s = mm(split[...], twice[y], ((1,), (1,))) + c2
            soft = jnp.maximum(jnp.log2(1.0 + jnp.exp2(jnp.minimum(s, 126.0))), s)
            power = s - soft
            if masked:
                row = iota((TALL, ROWS), 0)
                row = (row % ROWS) + (row // ROWS) * (NY * ROWS)
                first = ((c * PAIR - mine) * NY + col - y) * ROWS
                allowed = iota((TALL, ROWS), 1) - row < first
                soft = jnp.where(allowed, soft, 0.0)
            rounded = soft.astype(bf16)
            later = mm(rounded, upper[...])
            weight = jnp.exp2(power - (later + carry))
            if masked:
                weight = jnp.where(allowed, weight, 0.0)
            total = total + mm(weight.astype(bf16), local[y, :, SD:])
            carry = carry + (later[:, :1] + rounded[:, :1].astype(f32))
        acc[...] = total
        car[...] = jnp.broadcast_to(carry, (TALL, SD))
        for k in range(PAIR):
            rows = slice(k * ROWS, (k + 1) * ROWS)
            out[c * PAIR + k, :ROWS, :] = acc[rows, :].astype(bf16)
            wide = jnp.transpose(car[rows, :])[:8, :]
            a, b = wide[:, :SD], wide[:, SD:]
            ha, hb = a.astype(bf16).astype(f32), b.astype(bf16).astype(f32)
            row = iota((8, SD), 0)
            low = jnp.where(row == 2, a - ha, jnp.where(row == 3, b - hb, 0.0))
            packed = jnp.where(row == 0, ha, jnp.where(row == 1, hb, low))
            out[c * PAIR + k, ROWS:, :] = packed.astype(bf16)

    own = mine // PAIR

    def nothing(z, _):
        out[z, :, :] = jnp.zeros((ROWS + 8, SD), bf16)
        return 0

    def full(c, _):
        rows_of(c, False)
        return 0

    lax.fori_loop(0, own * PAIR, nothing, 0)
    rows_of(own, True)
    lax.fori_loop(own + 1, NZ // PAIR, full, 0)


def join_kernel(parts, total, squares):
    rows = []
    run = jnp.zeros((1, ROWS), f32)
    for i in reversed(range(NZ)):
        rows.append(jnp.exp2(-run))
        p = parts[i, ROWS:, :].astype(f32)
        run = run + jnp.concatenate([p[0:1] + p[2:3], p[1:2] + p[3:4]], axis=1)
    factors = jnp.concatenate(rows + [jnp.zeros((SD - NZ, ROWS), f32)], axis=0)
    factors = jnp.transpose(factors)
    out = jnp.zeros((ROWS, SD), f32)
    for k, i in enumerate(reversed(range(NZ))):
        out = out + factors[:, k : k + 1] * parts[i, :ROWS, :].astype(f32)
    total[...] = out
    own = jnp.sum(out * out, axis=1, keepdims=True)
    row = jnp.transpose(jnp.broadcast_to(own, (ROWS, SD)))[:8, :]
    for t in range(8):
        squares[t, :, :] = row


def retain_kernel(lam, tq, inner, entering, gain, out):
    slices = entering[...].reshape(2 * RD, SD)
    state = [mm(spread(h), slices, ((0,), (0,))).astype(bf16) for h in range(2)]
    state = jnp.concatenate(state, axis=1)
    steps = (iota((ROWS, RD), 0) + 1).astype(f32)
    value = inner[...] + mm(tq[...], state) * jnp.exp(lam[0] * steps)
    value = value - jnp.mean(value, axis=1, keepdims=True)
    value = value * lax.rsqrt(jnp.mean(value * value, axis=1, keepdims=True) + epsilon)
    out[...] = (value * gain[...]).astype(bf16)


def output_kernel(total, squares, gain, ret, weights, out):
    mean = jnp.zeros((8, ROWS), f32)
    for t in range(8):
        mean = mean + squares[t]
    scale = lax.rsqrt(mean / STICK_WIDTH + epsilon)
    scale = jnp.concatenate([scale] * (SD // 8), axis=0)
    scale = jnp.transpose(scale)
    stick = (total[...] * scale * gain[...]).astype(bf16)
    both = jnp.concatenate([stick, ret[...]], axis=1)
    for n in range(8):
        cols = slice(n * 256, (n + 1) * 256)
        block = jnp.concatenate(
            [
                jnp.concatenate([weights[y, n, 32 * b : 32 * b + 32, :] for y in range(NY)], axis=0)
                for b in range(3)
            ],
            axis=1,
        )
        part = mm(both, block, ((1,), (1,))).astype(bf16)
        for t in range(8):
            out[t % 2, t // 2, :, cols] = part[t * 32 : (t + 1) * 32, :]


def to_all(x, axis):
    return lax.all_to_all(x, axis, 0, 0, tiled=True)


def body(
    inputs,
    input_gain,
    stick_query_w,
    stick_key_w,
    stick_value_w,
    ret_query_w,
    ret_key_w,
    ret_value_w,
    stick_offset,
    ret_log_decay,
    initial_state,
    stick_gain,
    ret_gain,
    stick_out_w,
    ret_out_w,
):
    sds = jax.ShapeDtypeStruct
    z, y, core = lax.axis_index("z"), lax.axis_index("y"), lax.axis_index("c")
    pos = jnp.stack([z, y, core]).astype(jnp.int32)

    ret_cols = ret_out_w.T
    columns = jnp.concatenate([stick_out_w.T, ret_cols[:, :SD], ret_cols[:, SD:]], axis=0)

    piece = call(piece_kernel, sds((4, ROWS + 8, RD), bf16), [VMEM, VMEM], 1000, (), WHOLE)(
        inputs, input_gain
    )
    own = to_all(piece, "x")
    other = lax.ppermute(own, "c", [(0, 1), (1, 0)])

    position = ((z * NY + y) * ROWS + jnp.arange(ROWS, dtype=jnp.int32)).astype(f32)
    half = RD // 2
    inverse = rope_base ** (-jnp.arange(half, dtype=f32) / half)
    angles = position[:, None] * inverse[None, :]

    def work(width):
        return [
            pltpu.VMEM((D, 3 * width), bf16),
            pltpu.VMEM((ROWS, D), bf16),
            pltpu.VMEM((ROWS, 3 * width), f32),
            pltpu.SemaphoreType.DMA((3,)),
        ]

    kv, queries = call(
        stick_project_kernel,
        (sds((ROWS, 2 * SD), bf16), sds((NZ, ROWS + 96, SD), bf16)),
        [SMEM] + [VMEM] * 3 + [HBM] * 3,
        400000000,
        work(SD),
        WHOLE,
    )(pos, own, other, columns, stick_query_w, stick_key_w, stick_value_w)
    ret_project = call(
        ret_project_kernel,
        (sds((NZ * NY, 8, SD), bf16),) + (sds((ROWS, RD), bf16),) * 3,
        [SMEM, SMEM] + [VMEM] * 4 + [HBM] * 3,
        6000000000,
        work(RD),
        WHOLE,
    )
    cosine, sine = jnp.cos(angles), jnp.sin(angles)
    states, tq, tk, rv = ret_project(
        pos,
        ret_log_decay,
        own,
        other,
        cosine,
        sine,
        ret_query_w,
        ret_key_w,
        ret_value_w,
    )

    row_kv = lax.all_gather(kv, "y", axis=0)
    col_q = to_all(queries, "z")
    weights = lax.all_gather(col_q[:, ROWS:, :], "y", axis=0)

    first = initial_state.reshape(4, RD)
    first = jnp.concatenate([first[:, :SD], first[:, SD:]], axis=0)
    slices = call(scan_kernel, sds((NZ * NY, 8, SD), bf16), [SMEM, VMEM, VMEM], 1000000)(
        ret_log_decay, to_all(states, SP), first
    )
    entering = to_all(slices, SP)
    inner = call(inner_kernel, sds((ROWS, RD), f32), [SMEM] + [VMEM] * 3, 2000000000)(
        ret_log_decay, tq, tk, rv
    )

    stick = call(
        stick_kernel,
        sds((NZ, ROWS + 8, SD), bf16),
        [SMEM, SMEM, HBM, VMEM],
        4000000000,
        [
            pltpu.VMEM((ROWS, ROWS), bf16),
            pltpu.VMEM((NY, ROWS, 2 * SD), bf16),
            pltpu.VMEM((TALL, 2 * SD), bf16),
            pltpu.VMEM((TALL, SD), f32),
            pltpu.VMEM((TALL, SD), f32),
            pltpu.VMEM((NY, ROWS, 2 * SD), bf16),
            pltpu.SemaphoreType.DMA((NY,)),
        ],
        WHOLE,
    )
    parts = stick(pos, stick_offset, row_kv, col_q)
    parts, entering = lax.optimization_barrier((parts, entering))
    parts = to_all(parts, "z")

    total, squares = call(
        join_kernel,
        (sds((ROWS, SD), f32), sds((8, 8, ROWS), f32)),
        [VMEM],
        10000000,
    )(parts)
    squares = to_all(squares, TP)

    ret_normed = call(retain_kernel, sds((ROWS, RD), bf16), [SMEM] + [VMEM] * 4, 100000000)(
        ret_log_decay, tq, inner, entering, ret_gain[None, :]
    )

    out = call(
        output_kernel,
        sds((2, 4, 32, D), bf16),
        [VMEM] * 5,
        400000000,
    )(
        total, squares, stick_gain[None, :], ret_normed, weights
    )
    pair = to_all(out, "c").astype(f32).sum(axis=0).astype(bf16)
    layer = to_all(pair, "x").astype(f32).sum(axis=0)
    return layer.astype(bf16)


def solution(mesh):
    split = Mesh(mesh.devices.reshape(NZ, NY, 4, 2), ALL)
    in_specs = (
        P(SP, TP),
        P(TP),
        P(None, TP),
        P(None, TP),
        P(None, TP),
        P(None, TP),
        P(None, TP),
        P(None, TP),
        P(TP),
        P(TP),
        P(TP, SP, None),
        P(TP),
        P(TP),
        P(TP, SP),
        P(TP, SP),
    )
    return jax.shard_map(
        body, mesh=split, in_specs=in_specs, out_specs=P(ALL, None), check_vma=False
    )
```

```python
import jax
import jax.numpy as jnp
from jax import lax
from jax.experimental import pallas as pl
from jax.experimental.pallas import tpu as pltpu
from jax.sharding import Mesh
from jax.sharding import PartitionSpec as P


D = 2048
STICK_WIDTH = 1024
ROWS = 256
SD = 128
RD = 256
NZ = 8
NY = 8
LOG2E = 1.4426950408889634

SP = ("z", "y")
TP = ("x", "c")
ALL = ("z", "y", "x", "c")

epsilon = 1e-06
rope_base = 10000.0
bf16 = jnp.bfloat16
f32 = jnp.float32

WHOLE = 66 * 1000 * 1000

VMEM = pl.BlockSpec(memory_space=pltpu.VMEM)
SMEM = pl.BlockSpec(memory_space=pltpu.SMEM)
HBM = pl.BlockSpec(memory_space=pltpu.HBM)


def mm(a, b, dims=((1,), (0,))):
    return lax.dot_general(a, b, (dims, ((), ())), preferred_element_type=f32)


def iota(shape, dim):
    return lax.broadcasted_iota(jnp.int32, shape, dim)


def spread(h):
    r = iota((2 * RD, RD), 0)
    return ((r // 8 * 4 + r % 4 == iota((2 * RD, RD), 1)) & (r // 4 % 2 == h)).astype(f32).astype(bf16)


def call(kernel, out, in_specs, flops, scratch=(), limit=48 * 1024 * 1024):
    return pl.pallas_call(
        kernel,
        out_shape=out,
        in_specs=in_specs,
        out_specs=jax.tree.map(lambda _: VMEM, out),
        scratch_shapes=list(scratch),
        compiler_params=pltpu.CompilerParams(vmem_limit_bytes=limit),
        cost_estimate=pl.CostEstimate(flops=flops, bytes_accessed=1 << 20, transcendentals=0),
    )


def piece_kernel(inputs, gain, out):
    for x in range(4):
        out[x, :ROWS, :] = inputs[...]
        out[x, ROWS:, :] = jnp.broadcast_to(gain[...][None, :], (8, RD))


def three_products(pos, own, other, matrices, buf, scaled, sums, sems):
    width = buf.shape[1] // 3
    copies = [
        pltpu.make_async_copy(w, buf.at[:, k * width : (k + 1) * width], sems.at[k])
        for k, w in enumerate(matrices)
    ]
    for copy in copies:
        copy.start()
    squares = jnp.zeros((ROWS, RD), f32)
    for part, ref in ((pos[2], own), (1 - pos[2], other)):
        for x in range(4):
            raw = ref[x, :ROWS, :].astype(f32)
            gain = ref[x, ROWS : ROWS + 1, :].astype(f32)
            squares = squares + raw * raw
            col = pl.multiple_of((2 * x + part) * RD, RD)
            scaled[:, pl.ds(col, RD)] = (raw * gain).astype(bf16)
    ready = 0
    for left in range(0, 3 * width, RD):
        right = min(left + RD, 3 * width)
        while ready < 3 and ready * width < right:
            copies[ready].wait()
            ready += 1
        sums[:, left:right] = mm(scaled[...], buf[:, left:right])
    scale = lax.rsqrt(jnp.sum(squares, axis=1, keepdims=True) / D + epsilon)
    return [(sums[:, k * width : (k + 1) * width] * scale).astype(bf16) for k in range(3)]


def stick_project_kernel(pos, own, other, columns, wq, wk, wv, kv, queries, *work):
    query, key, value = three_products(pos, own, other, (wq, wk, wv), *work)
    kv[:, :SD] = key
    kv[:, SD:] = value
    for z in range(NZ):
        queries[z, :ROWS, :] = query
        queries[z, ROWS:, :] = columns[...]


def ret_project_kernel(
    pos, lam, own, other, cos, sin, wq, wk, wv, states, tq, tk, rv, *work
):
    query, key, value = three_products(pos, own, other, (wq, wk, wv), *work)
    rv[...] = value
    cosine, sine = cos[...], sin[...]
    half = RD // 2

    def turn(v):
        a, b = v[:, :half].astype(f32), v[:, half:].astype(f32)
        return jnp.concatenate([a * cosine - b * sine, b * cosine + a * sine], axis=1)

    tq[...] = turn(query).astype(bf16)
    key = turn(key) * (RD**-0.5)
    tk[...] = key.astype(bf16)
    left = (ROWS - 1 - iota((ROWS, RD), 0)).astype(f32)
    decayed = (key * jnp.exp(lam[0] * left)).astype(bf16)
    state = mm(decayed, value, ((0,), (0,))).astype(bf16)
    slices = mm(spread(0), state[:, :SD]) + mm(spread(1), state[:, SD:])
    states[...] = slices.astype(bf16).reshape(NZ * NY, 8, SD)


def inner_kernel(lam, tq, tk, rv, inner):
    gap = (iota((ROWS, ROWS), 0) - iota((ROWS, ROWS), 1)).astype(f32)
    decay = jnp.where(gap >= 0.0, jnp.exp(lam[0] * jnp.maximum(gap, 0.0)), 0.0)
    scores = mm(tq[...], tk[...], ((1,), (1,))) * decay
    inner[...] = mm(scores.astype(bf16), rv[...])


def scan_kernel(lam, states, first, out):
    step = jnp.exp(jnp.full((8, SD), lam[0] * ROWS, f32))
    run = first[...]
    for b in range(NZ * NY):
        out[b, :, :] = run.astype(bf16)
        run = run * step + states[b].astype(f32)


PAIR = 2
TALL = PAIR * ROWS


def stick_kernel(pos, off, kvs, zq, out, upper, twice, split, acc, car, local, sems):
    copies = [pltpu.make_async_copy(kvs.at[y], local.at[y], sems.at[y]) for y in range(NY)]
    for copy in copies:
        copy.start()
    mine, col = pos[0], pos[1]
    c1 = (SD**-0.5) * LOG2E
    c2 = off[0] * LOG2E
    upper[...] = (iota((ROWS, ROWS), 0) > iota((ROWS, ROWS), 1)).astype(f32).astype(bf16)
    for y in range(NY):
        copies[y].wait()
        twice[y, :, :SD] = local[y, :, :SD]
        twice[y, :, SD:] = local[y, :, :SD]

    def rows_of(c, masked):
        for k in range(PAIR):
            rows = slice(k * ROWS, (k + 1) * ROWS)
            q = zq[c * PAIR + k, :ROWS, :].astype(f32) * c1
            high = q.astype(bf16)
            split[rows, :SD] = high
            split[rows, SD:] = (q - high.astype(f32)).astype(bf16)
        carry = jnp.zeros((TALL, 1), f32)
        total = jnp.zeros((TALL, SD), f32)
        for y in reversed(range(NY)):
            s = mm(split[...], twice[y], ((1,), (1,))) + c2
            soft = jnp.maximum(jnp.log2(1.0 + jnp.exp2(jnp.minimum(s, 126.0))), s)
            power = s - soft
            if masked:
                row = iota((TALL, ROWS), 0)
                row = (row % ROWS) + (row // ROWS) * (NY * ROWS)
                first = ((c * PAIR - mine) * NY + col - y) * ROWS
                allowed = iota((TALL, ROWS), 1) - row < first
                soft = jnp.where(allowed, soft, 0.0)
            rounded = soft.astype(bf16)
            later = mm(rounded, upper[...])
            weight = jnp.exp2(power - (later + carry))
            if masked:
                weight = jnp.where(allowed, weight, 0.0)
            total = total + mm(weight.astype(bf16), local[y, :, SD:])
            carry = carry + (later[:, :1] + rounded[:, :1].astype(f32))
        acc[...] = total
        car[...] = jnp.broadcast_to(carry, (TALL, SD))
        for k in range(PAIR):
            rows = slice(k * ROWS, (k + 1) * ROWS)
            out[c * PAIR + k, :ROWS, :] = acc[rows, :].astype(bf16)
            wide = jnp.transpose(car[rows, :])[:8, :]
            a, b = wide[:, :SD], wide[:, SD:]
            ha, hb = a.astype(bf16).astype(f32), b.astype(bf16).astype(f32)
            row = iota((8, SD), 0)
            low = jnp.where(row == 2, a - ha, jnp.where(row == 3, b - hb, 0.0))
            packed = jnp.where(row == 0, ha, jnp.where(row == 1, hb, low))
            out[c * PAIR + k, ROWS:, :] = packed.astype(bf16)

    own = mine // PAIR

    def nothing(z, _):
        out[z, :, :] = jnp.zeros((ROWS + 8, SD), bf16)
        return 0

    def full(c, _):
        rows_of(c, False)
        return 0

    lax.fori_loop(0, own * PAIR, nothing, 0)
    rows_of(own, True)
    lax.fori_loop(own + 1, NZ // PAIR, full, 0)


def join_kernel(parts, total, squares):
    rows = []
    run = jnp.zeros((1, ROWS), f32)
    for i in reversed(range(NZ)):
        rows.append(jnp.exp2(-run))
        p = parts[i, ROWS:, :].astype(f32)
        run = run + jnp.concatenate([p[0:1] + p[2:3], p[1:2] + p[3:4]], axis=1)
    factors = jnp.concatenate(rows + [jnp.zeros((SD - NZ, ROWS), f32)], axis=0)
    factors = jnp.transpose(factors)
    out = jnp.zeros((ROWS, SD), f32)
    for k, i in enumerate(reversed(range(NZ))):
        out = out + factors[:, k : k + 1] * parts[i, :ROWS, :].astype(f32)
    total[...] = out
    own = jnp.sum(out * out, axis=1, keepdims=True)
    row = jnp.transpose(jnp.broadcast_to(own, (ROWS, SD)))[:8, :]
    for t in range(8):
        squares[t, :, :] = row


def retain_kernel(lam, tq, inner, entering, gain, out):
    slices = entering[...].reshape(2 * RD, SD)
    state = [mm(spread(h), slices, ((0,), (0,))).astype(bf16) for h in range(2)]
    state = jnp.concatenate(state, axis=1)
    steps = (iota((ROWS, RD), 0) + 1).astype(f32)
    value = inner[...] + mm(tq[...], state) * jnp.exp(lam[0] * steps)
    value = value - jnp.mean(value, axis=1, keepdims=True)
    value = value * lax.rsqrt(jnp.mean(value * value, axis=1, keepdims=True) + epsilon)
    out[...] = (value * gain[...]).astype(bf16)


def output_kernel(total, squares, gain, ret, weights, out):
    mean = jnp.zeros((8, ROWS), f32)
    for t in range(8):
        mean = mean + squares[t]
    scale = lax.rsqrt(mean / STICK_WIDTH + epsilon)
    scale = jnp.concatenate([scale] * (SD // 8), axis=0)
    scale = jnp.transpose(scale)
    stick = (total[...] * scale * gain[...]).astype(bf16)
    both = jnp.concatenate([stick, ret[...]], axis=1)
    for n in range(8):
        cols = slice(n * 256, (n + 1) * 256)
        block = jnp.concatenate(
            [
                jnp.concatenate([weights[y, n, 32 * b : 32 * b + 32, :] for y in range(NY)], axis=0)
                for b in range(3)
            ],
            axis=1,
        )
        part = mm(both, block, ((1,), (1,))).astype(bf16)
        for t in range(8):
            out[t % 2, t // 2, :, cols] = part[t * 32 : (t + 1) * 32, :]


def to_all(x, axis):
    return lax.all_to_all(x, axis, 0, 0, tiled=True)


def body(
    inputs,
    input_gain,
    stick_query_w,
    stick_key_w,
    stick_value_w,
    ret_query_w,
    ret_key_w,
    ret_value_w,
    stick_offset,
    ret_log_decay,
    initial_state,
    stick_gain,
    ret_gain,
    stick_out_w,
    ret_out_w,
):
    sds = jax.ShapeDtypeStruct
    z, y, core = lax.axis_index("z"), lax.axis_index("y"), lax.axis_index("c")
    pos = jnp.stack([z, y, core]).astype(jnp.int32)

    ret_cols = ret_out_w.T
    columns = jnp.concatenate([stick_out_w.T, ret_cols[:, :SD], ret_cols[:, SD:]], axis=0)

    piece = call(piece_kernel, sds((4, ROWS + 8, RD), bf16), [VMEM, VMEM], 1000, (), WHOLE)(
        inputs, input_gain
    )
    own = to_all(piece, "x")
    other = lax.ppermute(own, "c", [(0, 1), (1, 0)])

    position = ((z * NY + y) * ROWS + jnp.arange(ROWS, dtype=jnp.int32)).astype(f32)
    half = RD // 2
    inverse = rope_base ** (-jnp.arange(half, dtype=f32) / half)
    angles = position[:, None] * inverse[None, :]

    def work(width):
        return [
            pltpu.VMEM((D, 3 * width), bf16),
            pltpu.VMEM((ROWS, D), bf16),
            pltpu.VMEM((ROWS, 3 * width), f32),
            pltpu.SemaphoreType.DMA((3,)),
        ]

    kv, queries = call(
        stick_project_kernel,
        (sds((ROWS, 2 * SD), bf16), sds((NZ, ROWS + 96, SD), bf16)),
        [SMEM] + [VMEM] * 3 + [HBM] * 3,
        400000000,
        work(SD),
        WHOLE,
    )(pos, own, other, columns, stick_query_w, stick_key_w, stick_value_w)
    ret_project = call(
        ret_project_kernel,
        (sds((NZ * NY, 8, SD), bf16),) + (sds((ROWS, RD), bf16),) * 3,
        [SMEM, SMEM] + [VMEM] * 4 + [HBM] * 3,
        6000000000,
        work(RD),
        WHOLE,
    )
    cosine, sine = jnp.cos(angles), jnp.sin(angles)
    states, tq, tk, rv = ret_project(
        pos,
        ret_log_decay,
        own,
        other,
        cosine,
        sine,
        ret_query_w,
        ret_key_w,
        ret_value_w,
    )

    row_kv = lax.all_gather(kv, "y", axis=0)
    col_q = to_all(queries, "z")
    cut = col_q[:, ROWS:, :]
    weights = lax.all_gather(cut, "y", axis=0)

    first = initial_state.reshape(4, RD)
    first = jnp.concatenate([first[:, :SD], first[:, SD:]], axis=0)
    arrived = to_all(states, SP)
    slices = call(scan_kernel, sds((NZ * NY, 8, SD), bf16), [SMEM, VMEM, VMEM], 1000000)(
        ret_log_decay, arrived, first
    )
    entering = to_all(slices, SP)
    inner = call(inner_kernel, sds((ROWS, RD), f32), [SMEM] + [VMEM] * 3, 2000000000)(
        ret_log_decay, tq, tk, rv
    )

    stick = call(
        stick_kernel,
        sds((NZ, ROWS + 8, SD), bf16),
        [SMEM, SMEM, HBM, VMEM],
        4000000000,
        [
            pltpu.VMEM((ROWS, ROWS), bf16),
            pltpu.VMEM((NY, ROWS, 2 * SD), bf16),
            pltpu.VMEM((TALL, 2 * SD), bf16),
            pltpu.VMEM((TALL, SD), f32),
            pltpu.VMEM((TALL, SD), f32),
            pltpu.VMEM((NY, ROWS, 2 * SD), bf16),
            pltpu.SemaphoreType.DMA((NY,)),
        ],
        WHOLE,
    )
    parts = stick(pos, stick_offset, row_kv, col_q)
    parts, entering = lax.optimization_barrier((parts, entering))
    parts = to_all(parts, "z")

    total, squares = call(
        join_kernel,
        (sds((ROWS, SD), f32), sds((8, 8, ROWS), f32)),
        [VMEM],
        10000000,
    )(parts)
    squares, weights = lax.optimization_barrier((squares, weights))
    squares = to_all(squares, TP)

    ret_normed = call(retain_kernel, sds((ROWS, RD), bf16), [SMEM] + [VMEM] * 4, 100000000)(
        ret_log_decay, tq, inner, entering, ret_gain[None, :]
    )

    out = call(
        output_kernel,
        sds((2, 4, 32, D), bf16),
        [VMEM] * 5,
        400000000,
    )(
        total, squares, stick_gain[None, :], ret_normed, weights
    )
    pair = to_all(out, "c").astype(f32).sum(axis=0).astype(bf16)
    layer = to_all(pair, "x").astype(f32).sum(axis=0)
    return layer.astype(bf16)


def solution(mesh):
    split = Mesh(mesh.devices.reshape(NZ, NY, 4, 2), ALL)
    in_specs = (
        P(SP, TP),
        P(TP),
        P(None, TP),
        P(None, TP),
        P(None, TP),
        P(None, TP),
        P(None, TP),
        P(None, TP),
        P(TP),
        P(TP),
        P(TP, SP, None),
        P(TP),
        P(TP),
        P(TP, SP),
        P(TP, SP),
    )
    return jax.shard_map(
        body, mesh=split, in_specs=in_specs, out_specs=P(ALL, None), check_vma=False
    )
```

```python
import jax
import jax.numpy as jnp
from jax import lax
from jax.experimental import pallas as pl
from jax.experimental.pallas import tpu as pltpu
from jax.sharding import Mesh
from jax.sharding import PartitionSpec as P


D = 2048
STICK_WIDTH = 1024
ROWS = 256
SD = 128
RD = 256
NZ = 8
NY = 8
LOG2E = 1.4426950408889634

SP = ("z", "y")
TP = ("x", "c")
ALL = ("z", "y", "x", "c")

epsilon = 1e-06
rope_base = 10000.0
bf16 = jnp.bfloat16
f32 = jnp.float32

WHOLE = 66 * 1000 * 1000

VMEM = pl.BlockSpec(memory_space=pltpu.VMEM)
SMEM = pl.BlockSpec(memory_space=pltpu.SMEM)
HBM = pl.BlockSpec(memory_space=pltpu.HBM)


def mm(a, b, dims=((1,), (0,))):
    return lax.dot_general(a, b, (dims, ((), ())), preferred_element_type=f32)


def iota(shape, dim):
    return lax.broadcasted_iota(jnp.int32, shape, dim)


def spread(h):
    r = iota((2 * RD, RD), 0)
    return ((r // 8 * 4 + r % 4 == iota((2 * RD, RD), 1)) & (r // 4 % 2 == h)).astype(f32).astype(bf16)


def call(kernel, out, in_specs, flops, scratch=(), limit=48 * 1024 * 1024):
    return pl.pallas_call(
        kernel,
        out_shape=out,
        in_specs=in_specs,
        out_specs=jax.tree.map(lambda _: VMEM, out),
        scratch_shapes=list(scratch),
        compiler_params=pltpu.CompilerParams(vmem_limit_bytes=limit),
        cost_estimate=pl.CostEstimate(flops=flops, bytes_accessed=1 << 20, transcendentals=0),
    )


def piece_kernel(inputs, gain, out):
    for x in range(4):
        out[x, :ROWS, :] = inputs[...]
        out[x, ROWS:, :] = jnp.broadcast_to(gain[...][None, :], (8, RD))


def three_products(pos, own, other, matrices, buf, scaled, sums, sems):
    width = buf.shape[1] // 3
    copies = [
        pltpu.make_async_copy(w, buf.at[:, k * width : (k + 1) * width], sems.at[k])
        for k, w in enumerate(matrices)
    ]
    for copy in copies:
        copy.start()
    squares = jnp.zeros((ROWS, RD), f32)
    for part, ref in ((pos[2], own), (1 - pos[2], other)):
        for x in range(4):
            raw = ref[x, :ROWS, :].astype(f32)
            gain = ref[x, ROWS : ROWS + 1, :].astype(f32)
            squares = squares + raw * raw
            col = pl.multiple_of((2 * x + part) * RD, RD)
            scaled[:, pl.ds(col, RD)] = (raw * gain).astype(bf16)
    ready = 0
    for left in range(0, 3 * width, RD):
        right = min(left + RD, 3 * width)
        while ready < 3 and ready * width < right:
            copies[ready].wait()
            ready += 1
        sums[:, left:right] = mm(scaled[...], buf[:, left:right])
    scale = lax.rsqrt(jnp.sum(squares, axis=1, keepdims=True) / D + epsilon)
    return [(sums[:, k * width : (k + 1) * width] * scale).astype(bf16) for k in range(3)]


def stick_project_kernel(pos, own, other, columns, wq, wk, wv, kv, queries, *work):
    query, key, value = three_products(pos, own, other, (wq, wk, wv), *work)
    kv[:, :SD] = key
    kv[:, SD:] = value
    for z in range(NZ):
        queries[z, :ROWS, :] = query
        queries[z, ROWS:, :] = columns[...]


def ret_project_kernel(
    pos, lam, own, other, cos, sin, wq, wk, wv, states, tq, tk, rv, *work
):
    query, key, value = three_products(pos, own, other, (wq, wk, wv), *work)
    rv[...] = value
    cosine, sine = cos[...], sin[...]
    half = RD // 2

    def turn(v):
        a, b = v[:, :half].astype(f32), v[:, half:].astype(f32)
        return jnp.concatenate([a * cosine - b * sine, b * cosine + a * sine], axis=1)

    tq[...] = turn(query).astype(bf16)
    key = turn(key) * (RD**-0.5)
    tk[...] = key.astype(bf16)
    left = (ROWS - 1 - iota((ROWS, RD), 0)).astype(f32)
    decayed = (key * jnp.exp(lam[0] * left)).astype(bf16)
    state = mm(decayed, value, ((0,), (0,))).astype(bf16)
    slices = mm(spread(0), state[:, :SD]) + mm(spread(1), state[:, SD:])
    states[...] = slices.astype(bf16).reshape(NZ * NY, 8, SD)


def inner_kernel(lam, tq, tk, rv, inner):
    gap = (iota((ROWS, ROWS), 0) - iota((ROWS, ROWS), 1)).astype(f32)
    decay = jnp.where(gap >= 0.0, jnp.exp(lam[0] * jnp.maximum(gap, 0.0)), 0.0)
    scores = mm(tq[...], tk[...], ((1,), (1,))) * decay
    inner[...] = mm(scores.astype(bf16), rv[...])


def scan_kernel(lam, states, first, out):
    step = jnp.exp(jnp.full((8, SD), lam[0] * ROWS, f32))
    run = first[...]
    for b in range(NZ * NY):
        out[b, :, :] = run.astype(bf16)
        run = run * step + states[b].astype(f32)


PAIR = 2
TALL = PAIR * ROWS


def stick_kernel(pos, off, kvs, zq, out, upper, twice, split, acc, car):
    mine, col = pos[0], pos[1]
    c1 = (SD**-0.5) * LOG2E
    c2 = off[0] * LOG2E
    upper[...] = (iota((ROWS, ROWS), 0) > iota((ROWS, ROWS), 1)).astype(f32).astype(bf16)
    for y in range(NY):
        twice[y, :, :SD] = kvs[y, :, :SD]
        twice[y, :, SD:] = kvs[y, :, :SD]

    def rows_of(c, masked):
        for k in range(PAIR):
            rows = slice(k * ROWS, (k + 1) * ROWS)
            q = zq[c * PAIR + k, :ROWS, :].astype(f32) * c1
            high = q.astype(bf16)
            split[rows, :SD] = high
            split[rows, SD:] = (q - high.astype(f32)).astype(bf16)
        carry = jnp.zeros((TALL, 1), f32)
        total = jnp.zeros((TALL, SD), f32)
        for y in reversed(range(NY)):
            s = mm(split[...], twice[y], ((1,), (1,))) + c2
            soft = jnp.maximum(jnp.log2(1.0 + jnp.exp2(jnp.minimum(s, 126.0))), s)
            power = s - soft
            if masked:
                row = iota((TALL, ROWS), 0)
                row = (row % ROWS) + (row // ROWS) * (NY * ROWS)
                first = ((c * PAIR - mine) * NY + col - y) * ROWS
                allowed = iota((TALL, ROWS), 1) - row < first
                soft = jnp.where(allowed, soft, 0.0)
            rounded = soft.astype(bf16)
            later = mm(rounded, upper[...])
            weight = jnp.exp2(power - (later + carry))
            if masked:
                weight = jnp.where(allowed, weight, 0.0)
            total = total + mm(weight.astype(bf16), kvs[y, :, SD:])
            carry = carry + (later[:, :1] + rounded[:, :1].astype(f32))
        acc[...] = total
        car[...] = jnp.broadcast_to(carry, (TALL, SD))
        for k in range(PAIR):
            rows = slice(k * ROWS, (k + 1) * ROWS)
            out[c * PAIR + k, :ROWS, :] = acc[rows, :].astype(bf16)
            wide = jnp.transpose(car[rows, :])[:8, :]
            a, b = wide[:, :SD], wide[:, SD:]
            ha, hb = a.astype(bf16).astype(f32), b.astype(bf16).astype(f32)
            row = iota((8, SD), 0)
            low = jnp.where(row == 2, a - ha, jnp.where(row == 3, b - hb, 0.0))
            packed = jnp.where(row == 0, ha, jnp.where(row == 1, hb, low))
            out[c * PAIR + k, ROWS:, :] = packed.astype(bf16)

    own = mine // PAIR

    def nothing(z, _):
        out[z, :, :] = jnp.zeros((ROWS + 8, SD), bf16)
        return 0

    def full(c, _):
        rows_of(c, False)
        return 0

    lax.fori_loop(0, own * PAIR, nothing, 0)
    rows_of(own, True)
    lax.fori_loop(own + 1, NZ // PAIR, full, 0)


def join_kernel(parts, total, squares):
    rows = []
    run = jnp.zeros((1, ROWS), f32)
    for i in reversed(range(NZ)):
        rows.append(jnp.exp2(-run))
        p = parts[i, ROWS:, :].astype(f32)
        run = run + jnp.concatenate([p[0:1] + p[2:3], p[1:2] + p[3:4]], axis=1)
    factors = jnp.concatenate(rows + [jnp.zeros((SD - NZ, ROWS), f32)], axis=0)
    factors = jnp.transpose(factors)
    out = jnp.zeros((ROWS, SD), f32)
    for k, i in enumerate(reversed(range(NZ))):
        out = out + factors[:, k : k + 1] * parts[i, :ROWS, :].astype(f32)
    total[...] = out
    own = jnp.sum(out * out, axis=1, keepdims=True)
    row = jnp.transpose(jnp.broadcast_to(own, (ROWS, SD)))[:8, :]
    for t in range(8):
        squares[t, :, :] = row


def retain_kernel(lam, tq, inner, entering, gain, out):
    slices = entering[...].reshape(2 * RD, SD)
    state = [mm(spread(h), slices, ((0,), (0,))).astype(bf16) for h in range(2)]
    state = jnp.concatenate(state, axis=1)
    steps = (iota((ROWS, RD), 0) + 1).astype(f32)
    value = inner[...] + mm(tq[...], state) * jnp.exp(lam[0] * steps)
    value = value - jnp.mean(value, axis=1, keepdims=True)
    value = value * lax.rsqrt(jnp.mean(value * value, axis=1, keepdims=True) + epsilon)
    out[...] = (value * gain[...]).astype(bf16)


def output_kernel(total, squares, gain, ret, weights, out):
    mean = jnp.zeros((8, ROWS), f32)
    for t in range(8):
        mean = mean + squares[t]
    scale = lax.rsqrt(mean / STICK_WIDTH + epsilon)
    scale = jnp.concatenate([scale] * (SD // 8), axis=0)
    scale = jnp.transpose(scale)
    stick = (total[...] * scale * gain[...]).astype(bf16)
    both = jnp.concatenate([stick, ret[...]], axis=1)
    for n in range(8):
        cols = slice(n * 256, (n + 1) * 256)
        block = jnp.concatenate(
            [
                jnp.concatenate([weights[y, n, 32 * b : 32 * b + 32, :] for y in range(NY)], axis=0)
                for b in range(3)
            ],
            axis=1,
        )
        part = mm(both, block, ((1,), (1,))).astype(bf16)
        for t in range(8):
            out[t % 2, t // 2, :, cols] = part[t * 32 : (t + 1) * 32, :]


def to_all(x, axis):
    return lax.all_to_all(x, axis, 0, 0, tiled=True)


def body(
    inputs,
    input_gain,
    stick_query_w,
    stick_key_w,
    stick_value_w,
    ret_query_w,
    ret_key_w,
    ret_value_w,
    stick_offset,
    ret_log_decay,
    initial_state,
    stick_gain,
    ret_gain,
    stick_out_w,
    ret_out_w,
):
    sds = jax.ShapeDtypeStruct
    z, y, core = lax.axis_index("z"), lax.axis_index("y"), lax.axis_index("c")
    pos = jnp.stack([z, y, core]).astype(jnp.int32)

    ret_cols = ret_out_w.T
    columns = jnp.concatenate([stick_out_w.T, ret_cols[:, :SD], ret_cols[:, SD:]], axis=0)

    piece = call(piece_kernel, sds((4, ROWS + 8, RD), bf16), [VMEM, VMEM], 1000, (), WHOLE)(
        inputs, input_gain
    )
    own = to_all(piece, "x")
    other = lax.ppermute(own, "c", [(0, 1), (1, 0)])

    position = ((z * NY + y) * ROWS + jnp.arange(ROWS, dtype=jnp.int32)).astype(f32)
    half = RD // 2
    inverse = rope_base ** (-jnp.arange(half, dtype=f32) / half)
    angles = position[:, None] * inverse[None, :]

    def work(width):
        return [
            pltpu.VMEM((D, 3 * width), bf16),
            pltpu.VMEM((ROWS, D), bf16),
            pltpu.VMEM((ROWS, 3 * width), f32),
            pltpu.SemaphoreType.DMA((3,)),
        ]

    kv, queries = call(
        stick_project_kernel,
        (sds((ROWS, 2 * SD), bf16), sds((NZ, ROWS + 96, SD), bf16)),
        [SMEM] + [VMEM] * 3 + [HBM] * 3,
        400000000,
        work(SD),
        WHOLE,
    )(pos, own, other, columns, stick_query_w, stick_key_w, stick_value_w)
    ret_project = call(
        ret_project_kernel,
        (sds((NZ * NY, 8, SD), bf16),) + (sds((ROWS, RD), bf16),) * 3,
        [SMEM, SMEM] + [VMEM] * 4 + [HBM] * 3,
        6000000000,
        work(RD),
        WHOLE,
    )
    cosine, sine = jnp.cos(angles), jnp.sin(angles)
    states, tq, tk, rv = ret_project(
        pos,
        ret_log_decay,
        own,
        other,
        cosine,
        sine,
        ret_query_w,
        ret_key_w,
        ret_value_w,
    )

    row_kv = lax.all_gather(kv, "y", axis=0)
    col_q = to_all(queries, "z")
    cut = col_q[:, ROWS:, :]
    weights = lax.all_gather(cut, "y", axis=0)

    first = initial_state.reshape(4, RD)
    first = jnp.concatenate([first[:, :SD], first[:, SD:]], axis=0)
    arrived = to_all(states, SP)
    arrived, row_kv = lax.optimization_barrier((arrived, row_kv))
    slices = call(scan_kernel, sds((NZ * NY, 8, SD), bf16), [SMEM, VMEM, VMEM], 1000000)(
        ret_log_decay, arrived, first
    )
    entering = to_all(slices, SP)
    inner = call(inner_kernel, sds((ROWS, RD), f32), [SMEM] + [VMEM] * 3, 2000000000)(
        ret_log_decay, tq, tk, rv
    )

    stick = call(
        stick_kernel,
        sds((NZ, ROWS + 8, SD), bf16),
        [SMEM, SMEM, VMEM, VMEM],
        4000000000,
        [
            pltpu.VMEM((ROWS, ROWS), bf16),
            pltpu.VMEM((NY, ROWS, 2 * SD), bf16),
            pltpu.VMEM((TALL, 2 * SD), bf16),
            pltpu.VMEM((TALL, SD), f32),
            pltpu.VMEM((TALL, SD), f32),
        ],
    )
    parts = stick(pos, stick_offset, row_kv, col_q)
    parts, entering = lax.optimization_barrier((parts, entering))
    parts = to_all(parts, "z")

    total, squares = call(
        join_kernel,
        (sds((ROWS, SD), f32), sds((8, 8, ROWS), f32)),
        [VMEM],
        10000000,
    )(parts)
    squares, weights = lax.optimization_barrier((squares, weights))
    squares = to_all(squares, TP)

    ret_normed = call(retain_kernel, sds((ROWS, RD), bf16), [SMEM] + [VMEM] * 4, 100000000)(
        ret_log_decay, tq, inner, entering, ret_gain[None, :]
    )

    out = call(
        output_kernel,
        sds((2, 4, 32, D), bf16),
        [VMEM] * 5,
        400000000,
    )(
        total, squares, stick_gain[None, :], ret_normed, weights
    )
    pair = to_all(out, "c").astype(f32).sum(axis=0).astype(bf16)
    layer = to_all(pair, "x").astype(f32).sum(axis=0)
    return layer.astype(bf16)


def solution(mesh):
    split = Mesh(mesh.devices.reshape(NZ, NY, 4, 2), ALL)
    in_specs = (
        P(SP, TP),
        P(TP),
        P(None, TP),
        P(None, TP),
        P(None, TP),
        P(None, TP),
        P(None, TP),
        P(None, TP),
        P(TP),
        P(TP),
        P(TP, SP, None),
        P(TP),
        P(TP),
        P(TP, SP),
        P(TP, SP),
    )
    return jax.shard_map(
        body, mesh=split, in_specs=in_specs, out_specs=P(ALL, None), check_vma=False
    )
```
